512 devices in a mesh: sp: 32 (over z, x), tp: 16 (over y, core).
Axes of the slice: x: 4, y: 8, z: 8, core: 2. Of those that a mesh axis runs over, the one named last changes fastest.
Arguments:
- queries: bfloat16 [12288, 1024], P('sp', 'tp'), may hold values from -6 to 6
- keys: bfloat16 [12288, 1024], P('sp', 'tp'), may hold values from -6 to 6
- values: bfloat16 [12288, 1024], P('sp', 'tp'), may hold values from -6 to 6
- log_cum: float32 [16, 12288], P('tp'), as said below
- residual: bfloat16 [12288, 2048], P('sp', 'tp'), may hold values from -6 to 6
- out_gain: float32 [1024], replicated, may hold values from 0.1 to 1.9
- w_out: bfloat16 [1024, 2048], P(None, 'tp'), may hold values from -0.1875 to 0.1875
- ffn_gain: float32 [2048], replicated, may hold values from 0.1 to 1.9
- routes: int32 [12288, 2], P('sp'), may hold values from 0 to 63, all different within a row; in each aligned block of 384 rows (0 to 383, 384 to 767, ...) at most 24 rows name the same one
- route_weight: float32 [12288, 2], P('sp'), may hold values from 0.25 to 2
- sh_gate: bfloat16 [2048, 512], P(None, 'tp'), may hold values from -0.125 to 0.125
- sh_up: bfloat16 [2048, 512], P(None, 'tp'), may hold values from -0.125 to 0.125
- sh_down: bfloat16 [512, 2048], P(None, 'tp'), may hold values from -0.25 to 0.25
- exp_gate: bfloat16 [64, 2048, 512], P('sp', None, 'tp'), may hold values from -0.125 to 0.125
- exp_up: bfloat16 [64, 2048, 512], P('sp', None, 'tp'), may hold values from -0.125 to 0.125
- exp_down: bfloat16 [64, 512, 2048], P('sp', None, 'tp'), may hold values from -0.25 to 0.25
Outputs:
- result: bfloat16 [12288, 2048], P('sp', 'tp')
The draws below stay inside these ranges and needn't reach their ends.
Inputs may be any that keep to these rules, and one draw needn't show every extreme that they name: `routes`: in each aligned block of 384 rows no expert is named by more than 24 rows, a bound that some block reaches. `log_cum`: never rises along positions.
All inputs are finite; a program needn't handle non-finite values.
Results may differ from the reference program's by a relative error of at most 0.0095.
Values may be sent and summed in bfloat16 or wider, within the bound.
No kernel may reach another device: no remote copies, remote signals or barrier semaphores. Data moves between devices by JAX's collectives and lax.ppermute only.
A program may use at most 64 MiB of HBM per device.

```python
import math
import jax
import jax.numpy as jnp
import numpy as np
from jax import lax

D = 2048
HEADS = 16
HEAD_DIM = 64
FE = 512
FS = 512
TOP_K = 2
TOK_DEV = 384
EXPERTS = 64
TOKENS = 12288
CAP = 24
N_SP = 32


def planted(key):
    first = jnp.clip(jax.random.normal(jax.random.fold_in(key, 11), (TOKENS, HEADS * HEAD_DIM), jnp.float32), -5.0, 5.0)
    second = jnp.clip(jax.random.normal(jax.random.fold_in(key, 12), (TOKENS, HEADS * HEAD_DIM), jnp.float32), -5.0, 5.0)
    return (first, second)


def draw_queries(key, part):
    return planted(key)[0].astype(jnp.bfloat16)


def draw_keys(key, part):
    return planted(key)[1].astype(jnp.bfloat16)


def draw_log_cum(key, part):
    slow_share = 0.5
    slow = jax.random.uniform(jax.random.fold_in(key, 21), (HEADS, 1)) < slow_share
    slow_total = jax.random.uniform(jax.random.fold_in(key, 22), (HEADS, 1), minval=0.3, maxval=1.2)
    fast_span = jnp.exp(jax.random.uniform(jax.random.fold_in(key, 23), (HEADS, 1), minval=jnp.log(30.0), maxval=jnp.log(100.0)))
    per_step = jnp.where(slow, slow_total / TOKENS, 1.0 / fast_span)
    block_factor = jnp.exp(jax.random.uniform(jax.random.fold_in(key, 24), (HEADS, TOKENS // TOK_DEV, 1), minval=jnp.log(0.4), maxval=jnp.log(2.5)))
    rough = jax.random.uniform(jax.random.fold_in(key, 25), (HEADS, TOKENS // TOK_DEV, TOK_DEV), minval=0.5, maxval=1.5)
    gate_steps = (per_step[:, :, None] * block_factor * rough).reshape(HEADS, TOKENS)
    return -jnp.cumsum(gate_steps, axis=1)


def shard_levels(own_key, dims, pieces, low, largest):
    factor_of = 1.0
    for dim, shards_of in pieces:
        draws = jax.random.uniform(jax.random.fold_in(jax.random.fold_in(own_key, 6), dim), (shards_of,), jnp.float32, low / len(pieces), largest / len(pieces))
        factor_of = factor_of * jnp.repeat(jnp.exp(draws), dims[dim] // shards_of).reshape((-1,) + (1,) * (len(dims) - 1 - dim))
    return factor_of


def deal_out(key, own, number, rows, amount, top, bound, lean):
    order = jax.random.permutation(key, amount)
    heavy_load, usual = portions_of(amount, rows * top, bound, lean, True), portions_of(amount, rows * top, bound, lean, False)
    places = jnp.arange(amount)

    def named(sizes, turn):
        used = int((sizes > 0).sum())
        fixed = max(1, used // 4)
        shifted = fixed + (places - fixed + turn * (used - fixed)) % max(1, amount - fixed)
        return jnp.zeros((amount,), jnp.int32).at[order[jnp.where(places < fixed, places, shifted)]].set(jnp.asarray(sizes, jnp.int32))

    sizes = jnp.where(number % 4 == 0, named(heavy_load, number // 4), named(usual, number - number // 4 - 1))
    mixed = jax.random.permutation(jax.random.fold_in(own, 3), amount)
    giver, sink = mixed[0:amount // 2 * 2:2], mixed[1:amount // 2 * 2:2]
    room = jnp.minimum(sizes[giver] - 1, bound - sizes[sink]) // 2
    room = jnp.where((giver == order[0]) | (sink == order[0]) | (sizes[sink] == 0), 0, jnp.maximum(room, 0))
    shifted = jax.random.randint(jax.random.fold_in(own, 4), (amount // 2,), 0, 1 << 20) % (room + 1)
    sizes = sizes.at[giver].add(-shifted).at[sink].add(shifted)
    items = jnp.searchsorted(jnp.cumsum(sizes), jnp.arange(rows * top), side="right").astype(jnp.int32)
    grid = items.reshape(top, rows).T
    grid = grid[jax.random.permutation(jax.random.fold_in(own, 1), rows)]
    turn = jax.random.randint(jax.random.fold_in(own, 2), (rows, 1), 0, top)
    return jnp.take_along_axis(grid, (jnp.arange(top)[None, :] + turn) % top, axis=1)


def portions_of(count, total, bound, lean, full):
    loads = [(1 << 20) // math.isqrt(grade ** lean) + 1 for grade in range(1, count + 1)]
    largest = bound if full else min(bound, max(-(-total // count), total * loads[0] // sum(loads)))
    least = 1 if total - largest >= count - 1 else 0
    holding, spare = [largest] + [least] * (count - 1), total - largest - least * (count - 1)
    while spare > 0:
        free = [i for i in range(1, count) if holding[i] < largest] or [i for i in range(1, count) if holding[i] < bound]
        whole, left = sum([loads[i] for i in free]), spare
        for i in free:
            addition = min(bound - holding[i], max(1, left * loads[i] // whole), spare)
            holding[i] = holding[i] + addition
            spare = spare - addition
    return np.array(holding)


def centred(key, extent, width, bound, shards=(), kind=jnp.bfloat16):
    result = width * jax.random.normal(key, extent, jnp.float32)
    if shards:
        result = result * shard_levels(key, extent, shards, -0.22, 0.18)
    return jnp.clip(result, -bound, bound).astype(kind)


def setup_inputs(seed: int = 0) -> dict:
    splits = jax.random.split(jax.random.key(seed), 17)
    queries = draw_queries(jax.random.fold_in(splits[16], 71), 0)
    keys = draw_keys(jax.random.fold_in(splits[16], 71), 0)
    values = centred(splits[2], (TOKENS, HEADS * HEAD_DIM), 1.0, 6.0, ((0, 32), (1, 16)))
    log_cum = draw_log_cum(jax.random.fold_in(splits[16], 71), 0)
    residual = centred(splits[4], (TOKENS, D), 1.0, 6.0, ((0, 32), (1, 16)))
    out_gain = jnp.clip(1.0 + 0.18 * jax.random.normal(splits[5], (HEADS * HEAD_DIM,), jnp.float32), 0.1, 1.9)
    w_out = centred(splits[6], (HEADS * HEAD_DIM, D), (HEADS * HEAD_DIM) ** -0.5, 0.1875, ((1, 16),))
    ffn_gain = jnp.clip(1.0 + 0.18 * jax.random.normal(splits[7], (D,), jnp.float32), 0.1, 1.9)
    routes_keys = jax.random.split(jax.random.fold_in(splits[8], 1), TOKENS // TOK_DEV)
    routes_turns = jax.random.permutation(jax.random.fold_in(splits[8], 3), TOKENS // TOK_DEV)
    routes = jax.vmap(lambda own, number: deal_out(jax.random.fold_in(splits[8], 2), own, number, TOK_DEV, EXPERTS, TOP_K, CAP, 2))(routes_keys, routes_turns).reshape((TOKENS, TOP_K))
    route_weight = jnp.clip(0.25 + 1.75 * jax.random.uniform(splits[9], (TOKENS, TOP_K), jnp.float32) ** shard_levels(splits[9], (TOKENS, TOP_K), ((0, 32),), -0.2, 0.2), 0.25, 2.0)
    sh_gate = centred(splits[10], (D, FS), D ** -0.5, 0.125, ((1, 16),))
    sh_up = centred(splits[11], (D, FS), D ** -0.5, 0.125, ((1, 16),))
    sh_down = centred(splits[12], (FS, D), FS ** -0.5, 0.25, ((1, 16),))
    exp_gate = centred(splits[13], (EXPERTS, D, FE), D ** -0.5, 0.125, ((0, 32), (2, 16)))
    exp_up = centred(splits[14], (EXPERTS, D, FE), D ** -0.5, 0.125, ((0, 32), (2, 16)))
    exp_down = centred(splits[15], (EXPERTS, FE, D), FE ** -0.5, 0.25, ((0, 32), (2, 16)))
    return {"queries": queries, "keys": keys, "values": values, "log_cum": log_cum, "residual": residual, "out_gain": out_gain, "w_out": w_out, "ffn_gain": ffn_gain, "routes": routes, "route_weight": route_weight, "sh_gate": sh_gate, "sh_up": sh_up, "sh_down": sh_down, "exp_gate": exp_gate, "exp_up": exp_up, "exp_down": exp_down}


EPS = 1e-06

def rms_scaled(matrix, gain):
    floats = matrix.astype(jnp.float32)
    inverse = lax.rsqrt(lax.optimization_barrier(jnp.mean(floats * floats, axis=-1, keepdims=True)) + EPS)
    return (floats * inverse * gain.astype(jnp.float32)).astype(jnp.bfloat16)

def gated_hidden(gate, upward):
    return (jax.nn.silu(gate) * upward).astype(jnp.bfloat16)

def reference(queries, keys, values, log_cum, residual, out_gain, w_out, ffn_gain, routes, route_weight, sh_gate, sh_up, sh_down, exp_gate, exp_up, exp_down):
    scale = HEAD_DIM ** (-0.5)
    positions = jnp.arange(TOKENS, dtype=jnp.int32)

    def by_head(matrix):
        return jnp.transpose(matrix.reshape(TOKENS, HEADS, HEAD_DIM), (1, 0, 2))

    def one_head(inputs):
        query_head, key_head, value_head, cum_head = inputs

        def one_block(block):
            first = block * TOK_DEV
            query_block = lax.dynamic_slice_in_dim(query_head, first, TOK_DEV, 0)
            cum_block = lax.dynamic_slice_in_dim(cum_head, first, TOK_DEV, 0)
            score = jnp.dot(query_block, key_head.T, preferred_element_type=jnp.float32) * scale
            score = score + cum_block[:, None] - cum_head[None, :]
            causal = positions[None, :] <= (first + lax.iota(jnp.int32, TOK_DEV))[:, None]
            best = lax.optimization_barrier(jnp.max(jnp.where(causal, score, -jnp.inf), axis=1, keepdims=True))
            weight = jnp.where(causal, jnp.exp(score - best), 0.0)
            weighted = jnp.dot(weight.astype(jnp.bfloat16), value_head, preferred_element_type=jnp.float32)
            return (weighted / lax.optimization_barrier(jnp.sum(weight, axis=1, keepdims=True))).astype(jnp.bfloat16)
        blocks = lax.map(one_block, jnp.arange(N_SP, dtype=jnp.int32))
        return blocks.reshape(TOKENS, HEAD_DIM)
    heads_out = lax.map(one_head, (by_head(queries), by_head(keys), by_head(values), log_cum))
    heads_out = jnp.transpose(heads_out, (1, 0, 2)).reshape(TOKENS, HEADS * HEAD_DIM)
    mixed = rms_scaled(heads_out, out_gain)
    updated = (residual.astype(jnp.float32) + jnp.dot(mixed, w_out, preferred_element_type=jnp.float32)).astype(jnp.bfloat16)
    normed = rms_scaled(updated, ffn_gain)
    shared_hidden = gated_hidden(jnp.dot(normed, sh_gate, preferred_element_type=jnp.float32), jnp.dot(normed, sh_up, preferred_element_type=jnp.float32))
    shared_out = jnp.dot(shared_hidden, sh_down, preferred_element_type=jnp.float32)
    assigned = routes.reshape(N_SP, TOK_DEV * TOP_K)
    onehot = (assigned[:, :, None] == jnp.arange(EXPERTS, dtype=jnp.int32)[None, None, :]).astype(jnp.int32)
    slot_rank = lax.optimization_barrier(jnp.sum((jnp.cumsum(onehot, axis=1) - 1) * onehot, axis=2)).astype(jnp.int32)
    block_index = jnp.arange(N_SP, dtype=jnp.int32)[:, None]
    dest = ((assigned * N_SP + block_index) * CAP + slot_rank).reshape(-1).astype(jnp.int32)
    token_index = (block_index * TOK_DEV + jnp.arange(TOK_DEV * TOP_K, dtype=jnp.int32)[None, :] // TOP_K).reshape(-1)
    table = jnp.full((EXPERTS * N_SP * CAP,), TOKENS, jnp.int32).at[dest].set(token_index.astype(jnp.int32))
    padded = jnp.concatenate([normed, jnp.zeros((1, D), jnp.bfloat16)], axis=0)

    def one_expert(inputs):
        index_rows, weight_gate, weight_up, weight_down = inputs
        rows_in = padded[index_rows]
        hidden = gated_hidden(jnp.dot(rows_in, weight_gate, preferred_element_type=jnp.float32), jnp.dot(rows_in, weight_up, preferred_element_type=jnp.float32))
        return jnp.dot(hidden, weight_down, preferred_element_type=jnp.float32).astype(jnp.bfloat16)
    expert_out = lax.map(one_expert, (table.reshape(EXPERTS, N_SP * CAP), exp_gate, exp_up, exp_down))
    picked = expert_out.reshape(EXPERTS * N_SP * CAP, D)[dest].astype(jnp.float32)
    picked = picked * route_weight.reshape(-1)[:, None].astype(jnp.float32)
    routed = lax.optimization_barrier(jnp.sum(picked.reshape(TOKENS, TOP_K, D), axis=1))
    return (updated.astype(jnp.float32) + shared_out + routed).astype(jnp.bfloat16)
```

```python
import jax
import jax.numpy as jnp
from jax import lax
from jax.experimental import pallas as pl
from jax.experimental.pallas import tpu as pltpu
from jax.sharding import Mesh, PartitionSpec as P

EPS = 1e-06
LANES = 128
LOW = -1e30
PAD = 16
BF16 = jnp.bfloat16
F32 = jnp.float32
GRIDS = {32: (8, 4), 4: (2, 2), 8: (4, 2)}


def exchange(value, axis):
    return lax.all_to_all(value, axis, split_axis=0, concat_axis=0, tiled=True)


def copy_to_each(value, axis):
    return exchange(jnp.broadcast_to(value, (lax.axis_size(axis), *value.shape)), axis)


def three_parts(value):
    high = value.astype(BF16)
    rest = value - high.astype(F32)
    middle = rest.astype(BF16)
    low = (rest - middle.astype(F32)).astype(BF16)
    return [high, middle, low]


def attention_kernel(place, kv, query, cum, out, *, width, query_tile):
    zone, column = place[0], place[1]
    head = query.shape[1]
    count = query.shape[0]
    keys_each = kv.shape[2]
    total = count * width
    queries = jnp.concatenate([query[j] for j in range(count)], axis=1)
    ones = jnp.ones((PAD, total), BF16)
    queries = jnp.concatenate([queries, ones], axis=0)
    tiles = total // query_tile

    def step(block, state, masked):
        key_t = kv[block, :head, :]
        value_t = kv[block, head:, :]
        parts = three_parts(-cum[pl.ds(block, 1), :])
        filler = jnp.zeros((PAD - 3, keys_each), BF16)
        key_t = jnp.concatenate([key_t, *parts, filler], axis=0)
        result = []
        for i in range(tiles):
            best, total_weight, acc = state[i]
            part = queries[:, i * query_tile : (i + 1) * query_tile]
            score = lax.dot_general(
                key_t, part, (((0,), (0,)), ((), ())), preferred_element_type=F32
            )
            if masked:
                key_pos = column * width + lax.broadcasted_iota(jnp.int32, score.shape, 0)
                query_pos = i * query_tile + lax.broadcasted_iota(jnp.int32, score.shape, 1)
                score = jnp.where(key_pos <= query_pos, score, LOW)
            new_best = jnp.maximum(best, jnp.max(score, axis=0, keepdims=True))
            weight = jnp.exp(score - new_best)
            keep = jnp.exp(best - new_best)
            total_weight = total_weight * keep + jnp.sum(weight, axis=0, keepdims=True)
            acc = acc * keep + jnp.dot(
                value_t, weight.astype(BF16), preferred_element_type=F32
            )
            result.append((new_best, total_weight, acc))
        return tuple(result)

    start = tuple(
        (
            jnp.full((1, query_tile), LOW, F32),
            jnp.zeros((1, query_tile), F32),
            jnp.zeros((head, query_tile), F32),
        )
        for _ in range(tiles)
    )
    state = lax.fori_loop(0, zone, lambda block, s: step(block, s, False), start)
    state = step(zone, state, True)
    best = jnp.concatenate([s[0] for s in state], axis=1)
    weight = jnp.concatenate([s[1] for s in state], axis=1)
    acc = jnp.concatenate([s[2] for s in state], axis=1)
    normal = (acc / weight).astype(BF16)
    parts = three_parts(best + jnp.log(weight))
    full = jnp.concatenate([normal, *parts, jnp.zeros((PAD - 3, total), BF16)], axis=0)
    for j in range(count):
        out[j] = full[:, j * width : (j + 1) * width]


def partial_attention(place, kv, query, cum):
    count, head, width = query.shape
    total = count * width
    tile = 512 if total % 512 == 0 else width
    return pl.pallas_call(
        lambda *refs: attention_kernel(*refs, width=width, query_tile=tile),
        out_shape=jax.ShapeDtypeStruct((count, head + PAD, width), BF16),
        in_specs=[
            pl.BlockSpec(memory_space=pltpu.SMEM),
            pl.BlockSpec(memory_space=pltpu.VMEM),
            pl.BlockSpec(memory_space=pltpu.VMEM),
            pl.BlockSpec(memory_space=pltpu.VMEM),
        ],
        out_specs=pl.BlockSpec(memory_space=pltpu.VMEM),
        compiler_params=pltpu.CompilerParams(vmem_limit_bytes=40 * 1024 * 1024),
        name="partial_attention",
    )(place, kv, query, cum)


def rms_inverse(squares, count):
    return lax.rsqrt(squares / count + EPS)


def gated_hidden(gate, upward):
    return (jax.nn.silu(gate) * upward).astype(BF16)


def wide_shard(matrix):
    columns, rows = matrix.shape[-2], matrix.shape[-1]
    turned = jnp.swapaxes(matrix, -1, -2)
    split = turned.reshape(-1, rows, columns // LANES, LANES)
    return jnp.swapaxes(split, 1, 2).reshape(-1, LANES)


def joined_wide(pieces, hidden):
    shards = pieces.shape[0]
    blocks = pieces.reshape(shards, -1, hidden, LANES)
    return jnp.transpose(blocks, (0, 2, 1, 3)).reshape(shards * hidden, -1)


def joined_tall(pieces):
    shards, inner = pieces.shape[0], pieces.shape[1]
    return jnp.transpose(pieces, (1, 0, 2)).reshape(inner, shards * LANES)


def feed_forward(rows, gate, upward, down):
    across = (((1,), (1,)), ((), ()))
    hidden = gated_hidden(
        lax.dot_general(rows, gate, across, preferred_element_type=F32),
        lax.dot_general(rows, upward, across, preferred_element_type=F32),
    )
    return jnp.dot(hidden, down, preferred_element_type=F32).astype(BF16)


def per_device(
    queries,
    keys,
    values,
    log_cum,
    residual,
    out_gain,
    w_out,
    ffn_gain,
    routes,
    route_weight,
    sh_gate,
    sh_up,
    sh_down,
    exp_gate,
    exp_up,
    exp_down,
):
    width, head = queries.shape
    zones, columns = lax.axis_size("z"), lax.axis_size("x")
    shards = lax.axis_size("tp")
    blocks = zones * columns
    zone, column, shard = lax.axis_index("z"), lax.axis_index("x"), lax.axis_index("tp")
    features = shards * LANES
    hidden = sh_gate.shape[1]
    inner = hidden * shards
    local_experts = exp_gate.shape[0]
    teams = shards // local_experts

    scale = head ** (-0.5)
    key_value = jnp.concatenate([keys.T, values.T], axis=0)
    query = (queries.T.astype(F32) * scale).astype(BF16)
    key_value = copy_to_each(key_value, "z")
    query = copy_to_each(query, "x")
    cum = lax.dynamic_index_in_dim(
        log_cum.reshape(zones, columns, width), column, 1, keepdims=False
    )

    packed = jnp.concatenate(
        [
            wide_shard(exp_gate),
            wide_shard(exp_up),
            exp_down.reshape(-1, LANES),
            wide_shard(sh_gate),
            wide_shard(sh_up),
            sh_down,
        ],
        axis=0,
    )
    packed = lax.all_gather(packed, "tp", axis=0, tiled=False)

    place = jnp.stack([zone, column]).astype(jnp.int32)
    partial = partial_attention(place, key_value, query, cum)
    partial = exchange(partial, "x").astype(F32)
    level = partial[:, head] + partial[:, head + 1] + partial[:, head + 2]
    share = jnp.exp(level - jnp.max(level, axis=0, keepdims=True))
    share = share / jnp.sum(share, axis=0, keepdims=True)
    head_out = jnp.sum(partial[:, :head] * share[:, None], axis=0).astype(BF16)

    all_heads = lax.all_gather(head_out, "tp", axis=0, tiled=True).astype(F32)
    inverse = rms_inverse(jnp.sum(all_heads * all_heads, axis=0, keepdims=True), all_heads.shape[0])
    mixed = (all_heads * inverse * out_gain[:, None]).astype(BF16)
    attended = lax.dot_general(mixed, w_out, (((0,), (0,)), ((), ())), preferred_element_type=F32)
    updated = (residual.astype(F32) + attended).astype(BF16)

    top = routes.shape[1]
    experts = local_experts * blocks
    capacity = 2 * width * top // experts
    slots = experts * capacity
    chosen = [routes[:, k, None] == lax.iota(jnp.int32, experts)[None, :] for k in range(top)]
    named = sum(c.astype(BF16) for c in chosen)
    earlier = (lax.iota(jnp.int32, width)[:, None] > lax.iota(jnp.int32, width)[None, :]).astype(BF16)
    rank = jnp.dot(earlier, named, preferred_element_type=F32)
    picks = []
    for k in range(top):
        own = jnp.sum(jnp.where(chosen[k], rank, 0.0), axis=1).astype(jnp.int32)
        slot = routes[:, k] * capacity + own
        picks.append(slot[:, None] == lax.iota(jnp.int32, slots)[None, :])
    select = sum(p.astype(BF16) for p in picks)
    weights = sum(jnp.where(p, route_weight[:, k, None], 0.0) for k, p in enumerate(picks))
    weight_high = lax.reduce_precision(weights, 8, 7)
    weight_low = (weights - weight_high).astype(BF16)
    weight_high = weight_high.astype(BF16)

    outgoing = lax.dot_general(
        select, updated, (((0,), (0,)), ((), ())), preferred_element_type=F32
    ).astype(BF16)
    per_block = local_experts * capacity
    landed = exchange(outgoing.reshape(blocks, per_block, LANES), ("z", "x"))
    rounds = blocks // teams
    landed = landed.reshape(rounds, teams, local_experts, capacity, LANES)
    landed = jnp.transpose(landed, (2, 1, 0, 3, 4)).reshape(shards, rounds * capacity, LANES)
    routed_rows = rounds * capacity
    own_rows = width // shards
    mixed_rows = jnp.concatenate([landed, updated.reshape(shards, own_rows, LANES)], axis=1)
    rows = exchange(mixed_rows, "tp").astype(F32)
    inverse = rms_inverse(jnp.sum(rows * rows, axis=(0, 2), keepdims=True), features)
    normed = (rows * inverse * ffn_gain.reshape(shards, 1, LANES)).astype(BF16)
    normed = jnp.transpose(normed, (1, 0, 2)).reshape(routed_rows + own_rows, features)

    mine = shard // teams
    wide = features * hidden // LANES
    tall = inner
    at = 0

    def piece(base, size):
        return lax.dynamic_slice_in_dim(packed, base, size, 1)

    gate = joined_wide(piece(at + mine * wide, wide), hidden)
    at += local_experts * wide
    upward = joined_wide(piece(at + mine * wide, wide), hidden)
    at += local_experts * wide
    down = joined_tall(piece(at + mine * tall, tall))
    at += local_experts * tall
    shared_gate = joined_wide(packed[:, at : at + wide], hidden)
    at += wide
    shared_up = joined_wide(packed[:, at : at + wide], hidden)
    at += wide
    shared_down = joined_tall(packed[:, at : at + tall])

    routed_out = feed_forward(normed[:routed_rows], gate, upward, down)
    shared_out = feed_forward(normed[routed_rows:], shared_gate, shared_up, shared_down)
    returned = jnp.concatenate([routed_out, shared_out], axis=0)
    returned = jnp.transpose(returned.reshape(-1, shards, LANES), (1, 0, 2))
    returned = exchange(returned, "tp")
    shared = returned[:, routed_rows:].reshape(width, LANES).astype(F32)
    returned = returned[:, :routed_rows].reshape(local_experts, teams, rounds, capacity, LANES)
    returned = jnp.transpose(returned, (2, 1, 0, 3, 4)).reshape(blocks, per_block, LANES)
    answers = exchange(returned, ("z", "x")).reshape(slots, LANES)
    routed = jnp.dot(weight_high, answers, preferred_element_type=F32) + jnp.dot(
        weight_low, answers, preferred_element_type=F32
    )
    return (updated.astype(F32) + shared + routed).astype(BF16)


def solution(mesh):
    blocks, shards = mesh.devices.shape
    zones, columns = GRIDS[blocks]
    grid = Mesh(mesh.devices.reshape(zones, columns, shards), ("z", "x", "tp"))
    sp = ("z", "x")
    in_specs = (
        P(sp, "tp"),
        P(sp, "tp"),
        P(sp, "tp"),
        P("tp", None),
        P(sp, "tp"),
        P(),
        P(None, "tp"),
        P(),
        P(sp, None),
        P(sp, None),
        P(None, "tp"),
        P(None, "tp"),
        P(None, "tp"),
        P(sp, None, "tp"),
        P(sp, None, "tp"),
        P(sp, None, "tp"),
    )
    return jax.shard_map(
        per_device, mesh=grid, in_specs=in_specs, out_specs=P(sp, "tp"), check_vma=False
    )
```

```python
import jax
import jax.numpy as jnp
from jax import lax
from jax.experimental import pallas as pl
from jax.experimental.pallas import tpu as pltpu
from jax.sharding import Mesh, PartitionSpec as P


EPS = 1e-06
LANES = 128
LOW = -1e30
PAD = 16
BF16 = jnp.bfloat16
F32 = jnp.float32
GRIDS = {32: (8, 4), 4: (2, 2), 8: (4, 2)}


def exchange(value, axis):
    return lax.all_to_all(value, axis, split_axis=0, concat_axis=0, tiled=True)


def copy_to_each(value, axis):
    return exchange(jnp.broadcast_to(value, (lax.axis_size(axis), *value.shape)), axis)


def three_parts(value):
    high = value.astype(BF16)
    rest = value - high.astype(F32)
    middle = rest.astype(BF16)
    low = (rest - middle.astype(F32)).astype(BF16)
    return [high, middle, low]


def attention_kernel(place, kv, query, cum, out, *, width, query_tile):
    zone, column = place[0], place[1]
    head = query.shape[1]
    count = query.shape[0]
    keys_each = kv.shape[2]
    total = count * width
    queries = jnp.concatenate([query[j] for j in range(count)], axis=1)
    ones = jnp.ones((PAD, total), BF16)
    queries = jnp.concatenate([queries, ones], axis=0)
    tiles = total // query_tile

    def step(block, state, masked):
        key_t = kv[block, :head, :]
        value_t = kv[block, head:, :]
        parts = three_parts(-cum[pl.ds(block, 1), :])
        filler = jnp.zeros((PAD - 3, keys_each), BF16)
        key_t = jnp.concatenate([key_t, *parts, filler], axis=0)
        result = []
        for i in range(tiles):
            best, total_weight, acc = state[i]
            part = queries[:, i * query_tile : (i + 1) * query_tile]
            score = lax.dot_general(
                key_t, part, (((0,), (0,)), ((), ())), preferred_element_type=F32
            )
            if masked:
                key_pos = column * width + lax.broadcasted_iota(jnp.int32, score.shape, 0)
                query_pos = i * query_tile + lax.broadcasted_iota(jnp.int32, score.shape, 1)
                score = jnp.where(key_pos <= query_pos, score, LOW)
            new_best = jnp.maximum(best, jnp.max(score, axis=0, keepdims=True))
            weight = jnp.exp(score - new_best)
            keep = jnp.exp(best - new_best)
            total_weight = total_weight * keep + jnp.sum(weight, axis=0, keepdims=True)
            acc = acc * keep + jnp.dot(
                value_t, weight.astype(BF16), preferred_element_type=F32
            )
            result.append((new_best, total_weight, acc))
        return tuple(result)

    start = tuple(
        (
            jnp.full((1, query_tile), LOW, F32),
            jnp.zeros((1, query_tile), F32),
            jnp.zeros((head, query_tile), F32),
        )
        for _ in range(tiles)
    )
    state = lax.fori_loop(0, zone, lambda block, s: step(block, s, False), start)
    state = step(zone, state, True)
    best = jnp.concatenate([s[0] for s in state], axis=1)
    weight = jnp.concatenate([s[1] for s in state], axis=1)
    acc = jnp.concatenate([s[2] for s in state], axis=1)
    normal = (acc / weight).astype(BF16)
    parts = three_parts(best + jnp.log(weight))
    full = jnp.concatenate([normal, *parts, jnp.zeros((PAD - 3, total), BF16)], axis=0)
    for j in range(count):
        out[j] = full[:, j * width : (j + 1) * width]


def partial_attention(place, kv, query, cum):
    count, head, width = query.shape
    total = count * width
    tile = 512 if total % 512 == 0 else width
    return pl.pallas_call(
        lambda *refs: attention_kernel(*refs, width=width, query_tile=tile),
        out_shape=jax.ShapeDtypeStruct((count, head + PAD, width), BF16),
        in_specs=[
            pl.BlockSpec(memory_space=pltpu.SMEM),
            pl.BlockSpec(memory_space=pltpu.VMEM),
            pl.BlockSpec(memory_space=pltpu.VMEM),
            pl.BlockSpec(memory_space=pltpu.VMEM),
        ],
        out_specs=pl.BlockSpec(memory_space=pltpu.VMEM),
        compiler_params=pltpu.CompilerParams(vmem_limit_bytes=40 * 1024 * 1024),
        name="partial_attention",
    )(place, kv, query, cum)


def gated_hidden(gate, upward):
    return (jax.nn.silu(gate) * upward).astype(BF16)


def pack_kernel(*refs, shapes):
    sources, target, sem = refs[:-2], refs[-2], refs[-1]
    at = 0
    for source, shape in zip(sources, shapes):
        if len(shape) == 3:
            count, rows, columns = shape
            for e in range(count):
                for k in range(columns // LANES):
                    pltpu.make_async_copy(
                        source.at[e, :, pl.ds(k * LANES, LANES)],
                        target.at[pl.ds(at, rows), :],
                        sem,
                    ).start()
                    at += rows
        else:
            rows = shape[0]
            pltpu.make_async_copy(source, target.at[pl.ds(at, rows), :], sem).start()
            at += rows
    pltpu.make_async_copy(target, target, sem).wait()


def packed_shards(*sources):
    shapes = [source.shape for source in sources]
    total = sum(source.size for source in sources) // LANES
    return pl.pallas_call(
        lambda *refs: pack_kernel(*refs, shapes=shapes),
        out_shape=jax.ShapeDtypeStruct((total, LANES), BF16),
        in_specs=[pl.BlockSpec(memory_space=pltpu.HBM) for _ in sources],
        out_specs=pl.BlockSpec(memory_space=pltpu.HBM),
        scratch_shapes=[pltpu.SemaphoreType.DMA],
        name="pack_shards",
    )(*sources)


def feed_kernel(which, rows, gain, weights, out, gate, upward, *rest, first, count, experts):
    down, sems = rest if len(rest) == 2 else (None, rest[0])
    shards, hidden = gate.shape[0], gate.shape[1]
    inner = shards * hidden
    features = shards * LANES
    mine = which[0]
    wide = features * hidden // LANES
    bases = [mine * wide, (experts + mine) * wide, 2 * experts * wide + mine * inner]
    for n, target in enumerate((gate, upward)):
        base = pl.multiple_of(bases[n], hidden)
        for k in range(features // LANES):
            pltpu.make_async_copy(
                weights.at[:, pl.ds(base + k * hidden, hidden), :],
                target.at[:, :, pl.ds(k * LANES, LANES)],
                sems.at[n],
            ).start()
    base = pl.multiple_of(bases[2], hidden)
    for t in range(shards if down is not None else 0):
        pltpu.make_async_copy(
            weights.at[t, pl.ds(base, inner), :], down.at[:, pl.ds(t * LANES, LANES)], sems.at[2]
        ).start()

    floats = [rows[t, first : first + count, :].astype(F32) for t in range(shards)]
    squares = sum(f * f for f in floats)
    mean = jnp.sum(squares, axis=1, keepdims=True) / features
    inverse = lax.rsqrt(mean + EPS)
    normed = jnp.concatenate([(f * inverse * gain[t]).astype(BF16) for t, f in enumerate(floats)], axis=1)
    across = (((1,), (1,)), ((), ()))
    pltpu.make_async_copy(gate, gate, sems.at[0]).wait()
    first_half = lax.dot_general(
        normed, gate[...].reshape(inner, features), across, preferred_element_type=F32
    )
    pltpu.make_async_copy(upward, upward, sems.at[1]).wait()
    second_half = lax.dot_general(
        normed, upward[...].reshape(inner, features), across, preferred_element_type=F32
    )
    inside = gated_hidden(first_half, second_half)
    if down is None:
        out[...] = inside
        return
    pltpu.make_async_copy(down, down, sems.at[2]).wait()
    for t in range(shards):
        part = jnp.dot(inside, down[:, t * LANES : (t + 1) * LANES], preferred_element_type=F32)
        out[t] = part.astype(BF16)


def feed_forward(which, rows, gain, weights, hidden, first, count, experts, whole=True):
    shards = rows.shape[0]
    features = shards * LANES
    inner = shards * hidden
    shape = (shards, count, LANES) if whole else (count, inner)
    down = [pltpu.VMEM((inner, features), BF16)] if whole else []
    return pl.pallas_call(
        lambda *refs: feed_kernel(*refs, first=first, count=count, experts=experts),
        out_shape=jax.ShapeDtypeStruct(shape, BF16),
        in_specs=[
            pl.BlockSpec(memory_space=pltpu.SMEM),
            pl.BlockSpec(memory_space=pltpu.VMEM),
            pl.BlockSpec(memory_space=pltpu.VMEM),
            pl.BlockSpec(memory_space=pltpu.HBM),
        ],
        out_specs=pl.BlockSpec(memory_space=pltpu.VMEM),
        scratch_shapes=[
            pltpu.VMEM((shards, hidden, features), BF16),
            pltpu.VMEM((shards, hidden, features), BF16),
            *down,
            pltpu.SemaphoreType.DMA((3,)),
        ],
        compiler_params=pltpu.CompilerParams(vmem_limit_bytes=(54 if whole else 61) * 1024 * 1024),
    )(which, rows, gain, weights)


def per_device(
    queries,
    keys,
    values,
    log_cum,
    residual,
    out_gain,
    w_out,
    ffn_gain,
    routes,
    route_weight,
    sh_gate,
    sh_up,
    sh_down,
    exp_gate,
    exp_up,
    exp_down,
):
    width, head = queries.shape
    zones, columns = lax.axis_size("z"), lax.axis_size("x")
    shards = lax.axis_size("tp")
    blocks = zones * columns
    zone, column, shard = lax.axis_index("z"), lax.axis_index("x"), lax.axis_index("tp")
    hidden = sh_gate.shape[1]
    local_experts = exp_gate.shape[0]
    teams = shards // local_experts

    scale = head ** (-0.5)
    key_value = jnp.concatenate([keys.T, values.T], axis=0)
    key_value = copy_to_each(key_value, "z")
    query = (queries.T.astype(F32) * scale).astype(BF16)
    query = lax.all_gather(query, "x", axis=0, tiled=False)
    cum = lax.dynamic_index_in_dim(
        log_cum.reshape(zones, columns, width), column, 1, keepdims=False
    )
    expert_weights = packed_shards(
        jnp.swapaxes(exp_gate, 1, 2), jnp.swapaxes(exp_up, 1, 2), exp_down.reshape(-1, LANES)
    )
    expert_weights = lax.all_gather(expert_weights, "tp", axis=0, tiled=False)
    shared_weights = packed_shards(sh_gate.T[None], sh_up.T[None])
    shared_weights = lax.all_gather(shared_weights, "tp", axis=0, tiled=False)

    place = jnp.stack([zone, column]).astype(jnp.int32)
    partial = partial_attention(place, key_value, query, cum)
    partial = exchange(partial, "x").astype(F32)
    level = partial[:, head] + partial[:, head + 1] + partial[:, head + 2]
    share = jnp.exp(level - jnp.max(level, axis=0, keepdims=True))
    share = share / jnp.sum(share, axis=0, keepdims=True)
    head_out = jnp.sum(partial[:, :head] * share[:, None], axis=0).astype(BF16)

    all_heads = lax.all_gather(head_out, "tp", axis=0, tiled=True).astype(F32)
    mean = jnp.sum(all_heads * all_heads, axis=0, keepdims=True) / all_heads.shape[0]
    inverse = lax.rsqrt(mean + EPS)
    mixed = (all_heads * inverse * out_gain[:, None]).astype(BF16)
    attended = lax.dot_general(mixed, w_out, (((0,), (0,)), ((), ())), preferred_element_type=F32)
    updated = (residual.astype(F32) + attended).astype(BF16)

    top = routes.shape[1]
    experts = local_experts * blocks
    capacity = 2 * width * top // experts
    slots = experts * capacity
    chosen = [routes[:, k, None] == lax.iota(jnp.int32, experts)[None, :] for k in range(top)]
    named = sum(c.astype(BF16) for c in chosen)
    earlier = (lax.iota(jnp.int32, width)[:, None] > lax.iota(jnp.int32, width)[None, :]).astype(BF16)
    rank = jnp.dot(earlier, named, preferred_element_type=F32)
    picks = []
    for k in range(top):
        own = jnp.sum(jnp.where(chosen[k], rank, 0.0), axis=1).astype(jnp.int32)
        slot = routes[:, k] * capacity + own
        picks.append(slot[:, None] == lax.iota(jnp.int32, slots)[None, :])
    select = sum(p.astype(BF16) for p in picks)
    weights = sum(jnp.where(p, route_weight[:, k, None], 0.0) for k, p in enumerate(picks))
    weight_high = lax.reduce_precision(weights, 8, 7)
    weight_low = (weights - weight_high).astype(BF16)
    weight_high = weight_high.astype(BF16)

    outgoing = lax.dot_general(
        select, updated, (((0,), (0,)), ((), ())), preferred_element_type=F32
    ).astype(BF16)
    per_block = local_experts * capacity
    landed = exchange(outgoing.reshape(blocks, per_block, LANES), ("z", "x"))
    rounds = blocks // teams
    landed = landed.reshape(rounds, teams, local_experts, capacity, LANES)
    landed = jnp.transpose(landed, (2, 1, 0, 3, 4)).reshape(shards, rounds * capacity, LANES)
    routed_rows = rounds * capacity
    own_rows = width // shards
    mixed_rows = jnp.concatenate([landed, updated.reshape(shards, own_rows, LANES)], axis=1)
    rows = exchange(mixed_rows, "tp")
    gain = ffn_gain.reshape(shards, 1, LANES)
    mine = (shard // teams).astype(jnp.int32)[None]
    routed_out = feed_forward(
        mine, rows, gain, expert_weights, hidden, 0, routed_rows, local_experts
    )
    returned = exchange(routed_out, "tp")
    returned = returned.reshape(local_experts, teams, rounds, capacity, LANES)
    returned = jnp.transpose(returned, (2, 1, 0, 3, 4)).reshape(blocks, per_block, LANES)
    answers = exchange(returned, ("z", "x")).reshape(slots, LANES)
    share_hidden = feed_forward(
        jnp.zeros((1,), jnp.int32),
        rows,
        gain,
        shared_weights,
        hidden,
        routed_rows,
        own_rows,
        1,
        whole=False,
    )
    share_hidden = lax.all_gather(share_hidden, "tp", axis=0, tiled=True)
    shared = jnp.dot(share_hidden, sh_down, preferred_element_type=F32)
    routed = jnp.dot(weight_high, answers, preferred_element_type=F32) + jnp.dot(
        weight_low, answers, preferred_element_type=F32
    )
    return (updated.astype(F32) + shared + routed).astype(BF16)


def solution(mesh):
    blocks, shards = mesh.devices.shape
    zones, columns = GRIDS[blocks]
    grid = Mesh(mesh.devices.reshape(zones, columns, shards), ("z", "x", "tp"))
    sp = ("z", "x")
    in_specs = (
        P(sp, "tp"),
        P(sp, "tp"),
        P(sp, "tp"),
        P("tp", None),
        P(sp, "tp"),
        P(),
        P(None, "tp"),
        P(),
        P(sp, None),
        P(sp, None),
        P(None, "tp"),
        P(None, "tp"),
        P(None, "tp"),
        P(sp, None, "tp"),
        P(sp, None, "tp"),
        P(sp, None, "tp"),
    )
    return jax.shard_map(
        per_device, mesh=grid, in_specs=in_specs, out_specs=P(sp, "tp"), check_vma=False
    )
```

```python
import jax
import jax.numpy as jnp
from jax import lax
from jax.experimental import pallas as pl
from jax.experimental.pallas import tpu as pltpu
from jax.sharding import Mesh, PartitionSpec as P


EPS = 1e-06
LANES = 128
LOW = -1e30
PAD = 16
BF16 = jnp.bfloat16
F32 = jnp.float32
GRIDS = {32: (4, 2, 4), 4: (2, 1, 2), 8: (2, 2, 2)}


def exchange(value, axis):
    return lax.all_to_all(value, axis, split_axis=0, concat_axis=0, tiled=True)


def copy_to_each(value, axis):
    return exchange(jnp.broadcast_to(value, (lax.axis_size(axis), *value.shape)), axis)


def three_parts(value):
    high = value.astype(BF16)
    rest = value - high.astype(F32)
    middle = rest.astype(BF16)
    low = (rest - middle.astype(F32)).astype(BF16)
    return [high, middle, low]


def attention_kernel(place, kv, query, cum, out, key_rows, value_rows):
    team, own = place[0], place[1]
    teams, head, width = query.shape
    count = kv.shape[0]

    for b in range(count):
        parts = three_parts(-cum[:, b * width : (b + 1) * width])
        filler = jnp.zeros((LANES - head - 3, width), BF16)
        key_rows[b] = jnp.concatenate([kv[b, :head, :], *parts, filler], axis=0).T
        value_rows[b] = jnp.concatenate([kv[b, head:, :], jnp.ones((PAD, width), BF16)], axis=0)

    def step(block, part, state, masked):
        best, acc = state
        score = jnp.dot(key_rows[block], part, preferred_element_type=F32)
        if masked:
            key_pos = lax.broadcasted_iota(jnp.int32, score.shape, 0)
            query_pos = lax.broadcasted_iota(jnp.int32, score.shape, 1)
            score = jnp.where(key_pos <= query_pos, score, LOW)
        new_best = jnp.maximum(best, jnp.max(score, axis=0, keepdims=True))
        weight = jnp.exp(score - new_best).astype(BF16)
        added = jnp.dot(value_rows[block], weight, preferred_element_type=F32)
        return new_best, acc * jnp.exp(best - new_best) + added

    def fresh():
        return jnp.full((1, width), LOW, F32), jnp.zeros((head + PAD, width), F32)

    def extended(j):
        return jnp.concatenate([query[j], jnp.ones((LANES - head, width), BF16)], axis=0)

    def finish(j, states):
        best = states[0][0]
        for other, _ in states[1:]:
            best = jnp.maximum(best, other)
        acc = sum(a * jnp.exp(m - best) for m, a in states)
        total = acc[head : head + 1]
        parts = three_parts(best + jnp.log(total))
        out[j] = jnp.concatenate(
            [(acc[:head] / total).astype(BF16), *parts, jnp.zeros((PAD - 3, width), BF16)], axis=0
        )

    def full_tile(j, nothing):
        part = extended(j)

        def pair(i, states):
            return tuple(step(2 * i + n, part, s, False) for n, s in enumerate(states))

        finish(j, lax.fori_loop(0, count // 2, pair, (fresh(), fresh())))
        return nothing

    def empty_tile(j, nothing):
        out[j] = jnp.concatenate(
            [jnp.zeros((head, width), BF16), jnp.full((PAD, width), LOW, BF16)], axis=0
        )
        return nothing

    lax.fori_loop(0, team, empty_tile, 0)
    part = extended(team)
    state = lax.fori_loop(0, own, lambda b, s: step(b, part, s, False), fresh())
    finish(team, [step(own, part, state, True)])
    lax.fori_loop(team + 1, teams, full_tile, 0)


def partial_attention(place, kv, query, cum):
    teams, head, width = query.shape
    count = kv.shape[0]
    return pl.pallas_call(
        attention_kernel,
        out_shape=jax.ShapeDtypeStruct((teams, head + PAD, width), BF16),
        in_specs=[
            pl.BlockSpec(memory_space=pltpu.SMEM),
            pl.BlockSpec(memory_space=pltpu.VMEM),
            pl.BlockSpec(memory_space=pltpu.VMEM),
            pl.BlockSpec(memory_space=pltpu.VMEM),
        ],
        out_specs=pl.BlockSpec(memory_space=pltpu.VMEM),
        scratch_shapes=[
            pltpu.VMEM((count, width, LANES), BF16),
            pltpu.VMEM((count, head + PAD, width), BF16),
        ],
        compiler_params=pltpu.CompilerParams(vmem_limit_bytes=32 * 1024 * 1024),
        name="partial_attention",
    )(place, kv, query, cum)


def gated_hidden(gate, upward):
    return (jax.nn.silu(gate) * upward).astype(BF16)


def pack_kernel(*refs, shapes):
    sources, target = refs[:-1], refs[-1]
    at = 0
    for source, shape in zip(sources, shapes):
        if len(shape) == 3:
            count, rows, columns = shape
            for e in range(count):
                for k in range(columns // LANES):
                    target[at : at + rows, :] = source[e, :, k * LANES : (k + 1) * LANES]
                    at += rows
        else:
            rows = shape[0]
            target[at : at + rows, :] = source[...]
            at += rows


def packed_shards(*sources):
    shapes = [source.shape for source in sources]
    total = sum(source.size for source in sources) // LANES
    return pl.pallas_call(
        lambda *refs: pack_kernel(*refs, shapes=shapes),
        out_shape=jax.ShapeDtypeStruct((total, LANES), BF16),
        in_specs=[pl.BlockSpec(memory_space=pltpu.VMEM) for _ in sources],
        out_specs=pl.BlockSpec(memory_space=pltpu.VMEM),
        name="pack_shards",
    )(*sources)


def feed_kernel(which, rows, gain, weights, out, gate, upward, *rest, first, count, experts):
    down, sems = rest if len(rest) == 2 else (None, rest[0])
    shards, hidden = gate.shape[0], gate.shape[1]
    inner = shards * hidden
    features = shards * LANES
    mine = which[0]
    wide = features * hidden // LANES
    bases = [mine * wide, (experts + mine) * wide, 2 * experts * wide + mine * inner]
    for n, target in enumerate((gate, upward)):
        base = pl.multiple_of(bases[n], hidden)
        for k in range(features // LANES):
            pltpu.make_async_copy(
                weights.at[:, pl.ds(base + k * hidden, hidden), :],
                target.at[:, :, pl.ds(k * LANES, LANES)],
                sems.at[n],
            ).start()
    base = pl.multiple_of(bases[2], hidden)
    for t in range(shards if down is not None else 0):
        pltpu.make_async_copy(
            weights.at[t, pl.ds(base, inner), :], down.at[:, pl.ds(t * LANES, LANES)], sems.at[2]
        ).start()

    floats = [rows[t, first : first + count, :].astype(F32) for t in range(shards)]
    squares = sum(f * f for f in floats)
    mean = jnp.sum(squares, axis=1, keepdims=True) / features
    inverse = lax.rsqrt(mean + EPS)
    normed = jnp.concatenate([(f * inverse * gain[t]).astype(BF16) for t, f in enumerate(floats)], axis=1)
    across = (((1,), (1,)), ((), ()))
    pltpu.make_async_copy(gate, gate, sems.at[0]).wait()
    first_half = lax.dot_general(
        normed, gate[...].reshape(inner, features), across, preferred_element_type=F32
    )
    pltpu.make_async_copy(upward, upward, sems.at[1]).wait()
    second_half = lax.dot_general(
        normed, upward[...].reshape(inner, features), across, preferred_element_type=F32
    )
    inside = gated_hidden(first_half, second_half)
    if down is None:
        out[...] = inside
        return
    pltpu.make_async_copy(down, down, sems.at[2]).wait()
    for t in range(shards):
        part = jnp.dot(inside, down[:, t * LANES : (t + 1) * LANES], preferred_element_type=F32)
        out[t] = part.astype(BF16)


def feed_forward(which, rows, gain, weights, hidden, first, count, experts, whole=True):
    shards = rows.shape[0]
    features = shards * LANES
    inner = shards * hidden
    shape = (shards, count, LANES) if whole else (count, inner)
    down = [pltpu.VMEM((inner, features), BF16)] if whole else []
    return pl.pallas_call(
        lambda *refs: feed_kernel(*refs, first=first, count=count, experts=experts),
        out_shape=jax.ShapeDtypeStruct(shape, BF16),
        in_specs=[
            pl.BlockSpec(memory_space=pltpu.SMEM),
            pl.BlockSpec(memory_space=pltpu.VMEM),
            pl.BlockSpec(memory_space=pltpu.VMEM),
            pl.BlockSpec(memory_space=pltpu.HBM),
        ],
        out_specs=pl.BlockSpec(memory_space=pltpu.VMEM),
        scratch_shapes=[
            pltpu.VMEM((shards, hidden, features), BF16),
            pltpu.VMEM((shards, hidden, features), BF16),
            *down,
            pltpu.SemaphoreType.DMA((3,)),
        ],
        compiler_params=pltpu.CompilerParams(vmem_limit_bytes=(54 if whole else 61) * 1024 * 1024),
    )(which, rows, gain, weights)


def per_device(
    queries,
    keys,
    values,
    log_cum,
    residual,
    out_gain,
    w_out,
    ffn_gain,
    routes,
    route_weight,
    sh_gate,
    sh_up,
    sh_down,
    exp_gate,
    exp_up,
    exp_down,
):
    width, head = queries.shape
    near = ("zl", "x")
    whole = ("zh", "zl", "x")
    group = lax.axis_size(near)
    shards = lax.axis_size("tp")
    blocks = lax.axis_size(whole)
    team, own, shard = lax.axis_index("zh"), lax.axis_index(near), lax.axis_index("tp")
    hidden = sh_gate.shape[1]
    local_experts = exp_gate.shape[0]
    teams = shards // local_experts

    scale = head ** (-0.5)
    key_value = jnp.concatenate([keys.T, values.T], axis=0)
    key_value = copy_to_each(key_value, near)
    query = (queries.T.astype(F32) * scale).astype(BF16)
    query = lax.all_gather(query, "zh", axis=0, tiled=False)
    cum = lax.dynamic_slice_in_dim(log_cum, team * group * width, group * width, 1)
    expert_weights = packed_shards(
        jnp.swapaxes(exp_gate, 1, 2), jnp.swapaxes(exp_up, 1, 2), exp_down.reshape(-1, LANES)
    )
    expert_weights = lax.all_gather(expert_weights, "tp", axis=0, tiled=False)
    shared_weights = packed_shards(sh_gate.T[None], sh_up.T[None])
    shared_weights = lax.all_gather(shared_weights, "tp", axis=0, tiled=False)

    place = jnp.stack([team, own]).astype(jnp.int32)
    partial = partial_attention(place, key_value, query, cum)
    partial = exchange(partial, "zh").astype(F32)
    level = partial[:, head] + partial[:, head + 1] + partial[:, head + 2]
    share = jnp.exp(level - jnp.max(level, axis=0, keepdims=True))
    share = share / jnp.sum(share, axis=0, keepdims=True)
    head_out = jnp.sum(partial[:, :head] * share[:, None], axis=0).astype(BF16)

    all_heads = lax.all_gather(head_out[None], "tp", axis=0, tiled=True).astype(F32)
    channels = shards * head
    mean = jnp.sum(all_heads * all_heads, axis=(0, 1), keepdims=True) / channels
    inverse = lax.rsqrt(mean + EPS)
    mixed = (all_heads * inverse * out_gain.reshape(shards, head, 1)).astype(BF16).reshape(channels, width)
    attended = lax.dot_general(mixed, w_out, (((0,), (0,)), ((), ())), preferred_element_type=F32)
    updated = (residual.astype(F32) + attended).astype(BF16)

    top = routes.shape[1]
    experts = local_experts * blocks
    capacity = 2 * width * top // experts
    slots = experts * capacity
    chosen = [routes[:, k, None] == lax.iota(jnp.int32, experts)[None, :] for k in range(top)]
    named = sum(c.astype(BF16) for c in chosen)
    earlier = (lax.iota(jnp.int32, width)[:, None] > lax.iota(jnp.int32, width)[None, :]).astype(BF16)
    rank = jnp.dot(earlier, named, preferred_element_type=F32)
    picks = []
    for k in range(top):
        own = jnp.sum(jnp.where(chosen[k], rank, 0.0), axis=1).astype(jnp.int32)
        slot = routes[:, k] * capacity + own
        picks.append(slot[:, None] == lax.iota(jnp.int32, slots)[None, :])
    select = sum(p.astype(BF16) for p in picks)
    weights = sum(jnp.where(p, route_weight[:, k, None], 0.0) for k, p in enumerate(picks))
    weight_high = lax.reduce_precision(weights, 8, 7)
    weight_low = (weights - weight_high).astype(BF16)
    weight_high = weight_high.astype(BF16)

    outgoing = lax.dot_general(
        select, updated, (((0,), (0,)), ((), ())), preferred_element_type=F32
    ).astype(BF16)
    per_block = local_experts * capacity
    landed = exchange(outgoing.reshape(blocks, per_block, LANES), whole)
    rounds = blocks // teams
    landed = landed.reshape(rounds, teams, local_experts, capacity, LANES)
    landed = jnp.transpose(landed, (2, 1, 0, 3, 4)).reshape(shards, rounds * capacity, LANES)
    routed_rows = rounds * capacity
    own_rows = width // shards
    mixed_rows = jnp.concatenate([landed, updated.reshape(shards, own_rows, LANES)], axis=1)
    rows = exchange(mixed_rows, "tp")
    gain = ffn_gain.reshape(shards, 1, LANES)
    mine = (shard // teams).astype(jnp.int32)[None]
    routed_out = feed_forward(
        mine, rows, gain, expert_weights, hidden, 0, routed_rows, local_experts
    )
    returned = exchange(routed_out, "tp")
    returned = returned.reshape(local_experts, teams, rounds, capacity, LANES)
    returned = jnp.transpose(returned, (2, 1, 0, 3, 4)).reshape(blocks, per_block, LANES)
    answers = exchange(returned, whole).reshape(slots, LANES)
    share_hidden = feed_forward(
        jnp.zeros((1,), jnp.int32),
        rows,
        gain,
        shared_weights,
        hidden,
        routed_rows,
        own_rows,
        1,
        whole=False,
    )
    share_hidden = lax.all_gather(share_hidden, "tp", axis=0, tiled=True)
    shared = jnp.dot(share_hidden, sh_down, preferred_element_type=F32)
    routed = jnp.dot(weight_high, answers, preferred_element_type=F32) + jnp.dot(
        weight_low, answers, preferred_element_type=F32
    )
    return (updated.astype(F32) + shared + routed).astype(BF16)


def solution(mesh):
    blocks, shards = mesh.devices.shape
    grid = Mesh(mesh.devices.reshape(*GRIDS[blocks], shards), ("zh", "zl", "x", "tp"))
    sp = ("zh", "zl", "x")
    in_specs = (
        P(sp, "tp"),
        P(sp, "tp"),
        P(sp, "tp"),
        P("tp", None),
        P(sp, "tp"),
        P(),
        P(None, "tp"),
        P(),
        P(sp, None),
        P(sp, None),
        P(None, "tp"),
        P(None, "tp"),
        P(None, "tp"),
        P(sp, None, "tp"),
        P(sp, None, "tp"),
        P(sp, None, "tp"),
    )
    return jax.shard_map(
        per_device, mesh=grid, in_specs=in_specs, out_specs=P(sp, "tp"), check_vma=False
    )
```

```python
import jax
import jax.numpy as jnp
from jax import lax
from jax.experimental import pallas as pl
from jax.experimental.pallas import tpu as pltpu
from jax.sharding import Mesh, PartitionSpec as P


EPS = 1e-06
LANES = 128
LOW = -1e30
PAD = 16
BF16 = jnp.bfloat16
F32 = jnp.float32
GRIDS = {32: (4, 2, 4), 4: (2, 1, 2), 8: (2, 2, 2)}


def exchange(value, axis):
    return lax.all_to_all(value, axis, split_axis=0, concat_axis=0, tiled=True)


def copy_to_each(value, axis):
    return exchange(jnp.broadcast_to(value, (lax.axis_size(axis), *value.shape)), axis)


def three_parts(value):
    high = value.astype(BF16)
    rest = value - high.astype(F32)
    middle = rest.astype(BF16)
    low = (rest - middle.astype(F32)).astype(BF16)
    return [high, middle, low]


def attention_kernel(place, kv, query, cum, out, key_rows, value_rows):
    team, own = place[0], place[1]
    teams, head, width = query.shape
    count = kv.shape[0]

    for b in range(count):
        parts = three_parts(-cum[:, b * width : (b + 1) * width])
        filler = jnp.zeros((LANES - head - 3, width), BF16)
        key_rows[b] = jnp.concatenate([kv[b, :head, :], *parts, filler], axis=0).T
        value_rows[b] = jnp.concatenate([kv[b, head:, :], jnp.ones((PAD, width), BF16)], axis=0)

    def step(block, part, state, masked):
        best, acc = state
        score = jnp.dot(key_rows[block], part, preferred_element_type=F32)
        if masked:
            key_pos = lax.broadcasted_iota(jnp.int32, score.shape, 0)
            query_pos = lax.broadcasted_iota(jnp.int32, score.shape, 1)
            score = jnp.where(key_pos <= query_pos, score, LOW)
        new_best = jnp.maximum(best, jnp.max(score, axis=0, keepdims=True))
        weight = jnp.exp(score - new_best).astype(BF16)
        added = jnp.dot(value_rows[block], weight, preferred_element_type=F32)
        return new_best, acc * jnp.exp(best - new_best) + added

    def fresh():
        return jnp.full((1, width), LOW, F32), jnp.zeros((head + PAD, width), F32)

    def extended(j):
        turn = lax.rem(team - j + teams, teams)
        return jnp.concatenate([query[turn], jnp.ones((LANES - head, width), BF16)], axis=0)

    def finish(j, states):
        best = states[0][0]
        for other, _ in states[1:]:
            best = jnp.maximum(best, other)
        acc = sum(a * jnp.exp(m - best) for m, a in states)
        total = acc[head : head + 1]
        parts = three_parts(best + jnp.log(total))
        out[j] = jnp.concatenate(
            [(acc[:head] / total).astype(BF16), *parts, jnp.zeros((PAD - 3, width), BF16)], axis=0
        )

    def full_tile(j, nothing):
        part = extended(j)

        def pair(i, states):
            return tuple(step(2 * i + n, part, s, False) for n, s in enumerate(states))

        finish(j, lax.fori_loop(0, count // 2, pair, (fresh(), fresh())))
        return nothing

    def empty_tile(j, nothing):
        out[j] = jnp.concatenate(
            [jnp.zeros((head, width), BF16), jnp.full((PAD, width), LOW, BF16)], axis=0
        )
        return nothing

    lax.fori_loop(0, team, empty_tile, 0)
    part = extended(team)
    state = lax.fori_loop(0, own, lambda b, s: step(b, part, s, False), fresh())
    finish(team, [step(own, part, state, True)])
    lax.fori_loop(team + 1, teams, full_tile, 0)


def partial_attention(place, kv, query, cum):
    teams, head, width = query.shape
    count = kv.shape[0]
    return pl.pallas_call(
        attention_kernel,
        out_shape=jax.ShapeDtypeStruct((teams, head + PAD, width), BF16),
        in_specs=[
            pl.BlockSpec(memory_space=pltpu.SMEM),
            pl.BlockSpec(memory_space=pltpu.VMEM),
            pl.BlockSpec(memory_space=pltpu.VMEM),
            pl.BlockSpec(memory_space=pltpu.VMEM),
        ],
        out_specs=pl.BlockSpec(memory_space=pltpu.VMEM),
        scratch_shapes=[
            pltpu.VMEM((count, width, LANES), BF16),
            pltpu.VMEM((count, head + PAD, width), BF16),
        ],
        compiler_params=pltpu.CompilerParams(vmem_limit_bytes=32 * 1024 * 1024),
        name="partial_attention",
    )(place, kv, query, cum)


def gated_hidden(gate, upward):
    return (jax.nn.silu(gate) * upward).astype(BF16)


def pack_kernel(*refs, shapes):
    sources, target = refs[:-1], refs[-1]
    at = 0
    for source, shape in zip(sources, shapes):
        if len(shape) == 3:
            count, rows, columns = shape
            for e in range(count):
                for k in range(columns // LANES):
                    target[at : at + rows, :] = source[e, :, k * LANES : (k + 1) * LANES]
                    at += rows
        else:
            rows = shape[0]
            target[at : at + rows, :] = source[...]
            at += rows


def packed_shards(*sources):
    shapes = [source.shape for source in sources]
    total = sum(source.size for source in sources) // LANES
    return pl.pallas_call(
        lambda *refs: pack_kernel(*refs, shapes=shapes),
        out_shape=jax.ShapeDtypeStruct((total, LANES), BF16),
        in_specs=[pl.BlockSpec(memory_space=pltpu.VMEM) for _ in sources],
        out_specs=pl.BlockSpec(memory_space=pltpu.VMEM),
        name="pack_shards",
    )(*sources)


def feed_kernel(which, rows, gain, weights, out, gate, upward, down, sems, *, experts):
    shards, hidden = gate.shape[0], gate.shape[1]
    inner = shards * hidden
    features = shards * LANES
    mine = which[0]
    wide = features * hidden // LANES
    bases = [mine * wide, (experts + mine) * wide, 2 * experts * wide + mine * inner]
    for n, target in enumerate((gate, upward)):
        base = pl.multiple_of(bases[n], hidden)
        for k in range(features // LANES):
            pltpu.make_async_copy(
                weights.at[:, pl.ds(base + k * hidden, hidden), :],
                target.at[:, :, pl.ds(k * LANES, LANES)],
                sems.at[n],
            ).start()
    base = pl.multiple_of(bases[2], hidden)
    for t in range(shards):
        pltpu.make_async_copy(
            weights.at[t, pl.ds(base, inner), :], down.at[:, pl.ds(t * LANES, LANES)], sems.at[2]
        ).start()

    floats = [rows[t].astype(F32) for t in range(shards)]
    squares = sum(f * f for f in floats)
    mean = jnp.sum(squares, axis=1, keepdims=True) / features
    inverse = lax.rsqrt(mean + EPS)
    normed = jnp.concatenate([(f * inverse * gain[t]).astype(BF16) for t, f in enumerate(floats)], axis=1)
    across = (((1,), (1,)), ((), ()))
    pltpu.make_async_copy(gate, gate, sems.at[0]).wait()
    first_half = lax.dot_general(
        normed, gate[...].reshape(inner, features), across, preferred_element_type=F32
    )
    pltpu.make_async_copy(upward, upward, sems.at[1]).wait()
    second_half = lax.dot_general(
        normed, upward[...].reshape(inner, features), across, preferred_element_type=F32
    )
    inside = gated_hidden(first_half, second_half)
    pltpu.make_async_copy(down, down, sems.at[2]).wait()
    for t in range(shards):
        part = jnp.dot(inside, down[:, t * LANES : (t + 1) * LANES], preferred_element_type=F32)
        out[t] = part.astype(BF16)


def feed_forward(which, rows, gain, weights, hidden, experts):
    shards = rows.shape[0]
    features = shards * LANES
    inner = shards * hidden
    return pl.pallas_call(
        lambda *refs: feed_kernel(*refs, experts=experts),
        out_shape=jax.ShapeDtypeStruct(rows.shape, BF16),
        in_specs=[
            pl.BlockSpec(memory_space=pltpu.SMEM),
            pl.BlockSpec(memory_space=pltpu.VMEM),
            pl.BlockSpec(memory_space=pltpu.VMEM),
            pl.BlockSpec(memory_space=pltpu.HBM),
        ],
        out_specs=pl.BlockSpec(memory_space=pltpu.VMEM),
        scratch_shapes=[
            pltpu.VMEM((shards, hidden, features), BF16),
            pltpu.VMEM((shards, hidden, features), BF16),
            pltpu.VMEM((inner, features), BF16),
            pltpu.SemaphoreType.DMA((3,)),
        ],
        compiler_params=pltpu.CompilerParams(vmem_limit_bytes=52 * 1024 * 1024),
        name="routed_feed",
    )(which, rows, gain, weights)


def shared_kernel(rows, gain, gate, upward, out):
    shards = rows.shape[0]
    floats = [rows[t].astype(F32) for t in range(shards)]
    squares = sum(f * f for f in floats)
    inverse = lax.rsqrt(jnp.sum(squares, axis=1, keepdims=True) / (shards * LANES) + EPS)
    normed = jnp.concatenate([(f * inverse * gain[t]).astype(BF16) for t, f in enumerate(floats)], axis=1)
    across = (((1,), (1,)), ((), ()))
    out[...] = gated_hidden(
        lax.dot_general(gate[...], normed, across, preferred_element_type=F32),
        lax.dot_general(upward[...], normed, across, preferred_element_type=F32),
    )


def shared_feed(rows, gain, gate, upward):
    return pl.pallas_call(
        shared_kernel,
        out_shape=jax.ShapeDtypeStruct((gate.shape[0], rows.shape[1]), BF16),
        in_specs=[pl.BlockSpec(memory_space=pltpu.VMEM) for _ in range(4)],
        out_specs=pl.BlockSpec(memory_space=pltpu.VMEM),
        compiler_params=pltpu.CompilerParams(vmem_limit_bytes=24 * 1024 * 1024),
        name="shared_feed",
    )(rows, gain, gate, upward)


def per_device(
    queries,
    keys,
    values,
    log_cum,
    residual,
    out_gain,
    w_out,
    ffn_gain,
    routes,
    route_weight,
    sh_gate,
    sh_up,
    sh_down,
    exp_gate,
    exp_up,
    exp_down,
):
    width, head = queries.shape
    near = ("zl", "x")
    whole = ("zh", "zl", "x")
    group = lax.axis_size(near)
    shards = lax.axis_size("tp")
    blocks = lax.axis_size(whole)
    team, own, shard = lax.axis_index("zh"), lax.axis_index(near), lax.axis_index("tp")
    hidden = sh_gate.shape[1]
    local_experts = exp_gate.shape[0]
    owners = shards // local_experts

    scale = head ** (-0.5)
    key_value = jnp.concatenate([keys.T, values.T], axis=0)
    key_value = copy_to_each(key_value, near)
    query = (queries.T.astype(F32) * scale).astype(BF16)
    teams = lax.axis_size("zh")
    moved = [
        lax.ppermute(query, "zh", [(i, (i + n) % teams) for i in range(teams)])
        for n in range(1, teams)
    ]
    query = jnp.stack([query, *moved])
    cum = lax.dynamic_slice_in_dim(log_cum, team * group * width, group * width, 1)
    expert_weights = packed_shards(
        jnp.swapaxes(exp_gate, 1, 2), jnp.swapaxes(exp_up, 1, 2), exp_down.reshape(-1, LANES)
    )
    expert_weights = lax.all_gather(expert_weights, "tp", axis=0, tiled=False)

    place = jnp.stack([team, own]).astype(jnp.int32)
    partial = partial_attention(place, key_value, query, cum)
    partial = exchange(partial, "zh").astype(F32)
    level = partial[:, head] + partial[:, head + 1] + partial[:, head + 2]
    share = jnp.exp(level - jnp.max(level, axis=0, keepdims=True))
    share = share / jnp.sum(share, axis=0, keepdims=True)
    head_out = jnp.sum(partial[:, :head] * share[:, None], axis=0).astype(BF16)

    all_heads = lax.all_gather(head_out[None], "tp", axis=0, tiled=True).astype(F32)
    channels = shards * head
    mean = jnp.sum(all_heads * all_heads, axis=(0, 1), keepdims=True) / channels
    inverse = lax.rsqrt(mean + EPS)
    mixed = (all_heads * inverse * out_gain.reshape(shards, head, 1)).astype(BF16).reshape(channels, width)
    attended = lax.dot_general(mixed, w_out, (((0,), (0,)), ((), ())), preferred_element_type=F32)
    updated = (residual.astype(F32) + attended).astype(BF16)
    all_rows = lax.all_gather(updated[None], "tp", axis=0, tiled=True)

    top = routes.shape[1]
    experts = local_experts * blocks
    capacity = 2 * width * top // experts
    slots = experts * capacity
    chosen = [routes[:, k, None] == lax.iota(jnp.int32, experts)[None, :] for k in range(top)]
    named = sum(c.astype(BF16) for c in chosen)
    earlier = (lax.iota(jnp.int32, width)[:, None] > lax.iota(jnp.int32, width)[None, :]).astype(BF16)
    rank = jnp.dot(earlier, named, preferred_element_type=F32)
    picks = []
    for k in range(top):
        own = jnp.sum(jnp.where(chosen[k], rank, 0.0), axis=1).astype(jnp.int32)
        slot = routes[:, k] * capacity + own
        picks.append(slot[:, None] == lax.iota(jnp.int32, slots)[None, :])
    select = sum(p.astype(BF16) for p in picks)
    weights = sum(jnp.where(p, route_weight[:, k, None], 0.0) for k, p in enumerate(picks))
    weight_high = lax.reduce_precision(weights, 8, 7)
    weight_low = (weights - weight_high).astype(BF16)
    weight_high = weight_high.astype(BF16)

    outgoing = lax.dot_general(
        select, updated, (((0,), (0,)), ((), ())), preferred_element_type=F32
    ).astype(BF16)
    per_block = local_experts * capacity
    landed = exchange(outgoing.reshape(blocks, per_block, LANES), whole)
    rounds = blocks // owners
    landed = landed.reshape(rounds, owners, local_experts, capacity, LANES)
    landed = jnp.transpose(landed, (2, 1, 0, 3, 4)).reshape(shards, rounds * capacity, LANES)
    rows = exchange(landed, "tp")
    gain = ffn_gain.reshape(shards, 1, LANES)
    mine = (shard // owners).astype(jnp.int32)[None]
    routed_out = feed_forward(mine, rows, gain, expert_weights, hidden, local_experts)
    returned = exchange(routed_out, "tp")
    returned = returned.reshape(local_experts, owners, rounds, capacity, LANES)
    returned = jnp.transpose(returned, (2, 1, 0, 3, 4)).reshape(blocks, per_block, LANES)
    answers = exchange(returned, whole).reshape(slots, LANES)
    share_hidden = shared_feed(all_rows, gain, sh_gate.T, sh_up.T)
    share_hidden = lax.all_gather(share_hidden, "tp", axis=0, tiled=True)
    shared = lax.dot_general(
        share_hidden, sh_down, (((0,), (0,)), ((), ())), preferred_element_type=F32
    )
    routed = jnp.dot(weight_high, answers, preferred_element_type=F32) + jnp.dot(
        weight_low, answers, preferred_element_type=F32
    )
    return (updated.astype(F32) + shared + routed).astype(BF16)


def solution(mesh):
    blocks, shards = mesh.devices.shape
    grid = Mesh(mesh.devices.reshape(*GRIDS[blocks], shards), ("zh", "zl", "x", "tp"))
    sp = ("zh", "zl", "x")
    in_specs = (
        P(sp, "tp"),
        P(sp, "tp"),
        P(sp, "tp"),
        P("tp", None),
        P(sp, "tp"),
        P(),
        P(None, "tp"),
        P(),
        P(sp, None),
        P(sp, None),
        P(None, "tp"),
        P(None, "tp"),
        P(None, "tp"),
        P(sp, None, "tp"),
        P(sp, None, "tp"),
        P(sp, None, "tp"),
    )
    return jax.shard_map(
        per_device, mesh=grid, in_specs=in_specs, out_specs=P(sp, "tp"), check_vma=False
    )
```

```python
import jax
import jax.numpy as jnp
from jax import lax
from jax.experimental import pallas as pl
from jax.experimental.pallas import tpu as pltpu
from jax.sharding import Mesh, PartitionSpec as P


EPS = 1e-06
LANES = 128
LOW = -1e30
PAD = 16
CHAIN = 768
BF16 = jnp.bfloat16
F32 = jnp.float32
GRIDS = {32: (4, 2, 4), 4: (2, 1, 2), 8: (2, 2, 2)}


def exchange(value, axis):
    return lax.all_to_all(value, axis, split_axis=0, concat_axis=0, tiled=True)


def copy_to_each(value, axis):
    return exchange(jnp.broadcast_to(value, (lax.axis_size(axis), *value.shape)), axis)


def three_parts(value):
    high = value.astype(BF16)
    rest = value - high.astype(F32)
    middle = rest.astype(BF16)
    low = (rest - middle.astype(F32)).astype(BF16)
    return [high, middle, low]


def attention_kernel(place, kv, query, cum, out, key_rows, value_rows):
    team, own = place[0], place[1]
    teams, head, width = query.shape
    count = kv.shape[0]
    span = 2 * width
    reach = min(count, 8) * width
    piece = min(span, CHAIN)
    chains = span // piece

    for b in range(count):
        parts = three_parts(-cum[:, b * width : (b + 1) * width])
        filler = jnp.zeros((LANES - head - 3, width), BF16)
        key_rows[b * width : (b + 1) * width] = jnp.concatenate(
            [kv[b, :head, :], *parts, filler], axis=0
        ).T
        value_rows[:, b * width : (b + 1) * width] = jnp.concatenate(
            [kv[b, head:, :], jnp.ones((PAD, width), BF16)], axis=0
        )

    def step(i, part, state, limit):
        best, acc = state
        at = pl.ds(pl.multiple_of(i * reach, reach), reach)
        score = jnp.dot(key_rows[at, :], part, preferred_element_type=F32)
        if limit is not None:
            key_pos = i * reach + lax.broadcasted_iota(jnp.int32, score.shape, 0)
            score = jnp.where(key_pos <= limit, score, LOW)
        new_best = jnp.maximum(best, jnp.max(score, axis=0, keepdims=True))
        weight = jnp.exp(score - new_best).astype(BF16)
        added = jnp.dot(value_rows[:, at], weight, preferred_element_type=F32)
        return new_best, acc * jnp.exp(best - new_best) + added

    def run(tile, steps, masked):
        turns = [lax.rem(team - (2 * tile + n) + teams, teams) for n in range(2)]
        both = jnp.concatenate([query[turn] for turn in turns], axis=1)
        both = jnp.concatenate([both, jnp.ones((LANES - head, span), BF16)], axis=0)
        limits = [None] * chains
        if masked:
            lane = lax.broadcasted_iota(jnp.int32, (1, span), 1)
            block = 2 * tile + jnp.where(lane >= width, 1, 0)
            at = own * width + jnp.where(lane >= width, lane - width, lane)
            limit = jnp.where(block < team, -1, jnp.where(block == team, at, count * width))
            limits = [limit[:, c * piece : (c + 1) * piece] for c in range(chains)]
        parts = [both[:, c * piece : (c + 1) * piece] for c in range(chains)]
        first = tuple(
            (jnp.full((1, piece), LOW, F32), jnp.zeros((head + PAD, piece), F32)) for _ in range(chains)
        )
        states = lax.fori_loop(
            0,
            steps,
            lambda i, s: tuple(step(i, parts[c], s[c], limits[c]) for c in range(chains)),
            first,
        )
        best = jnp.concatenate([m for m, _ in states], axis=1)
        acc = jnp.concatenate([a for _, a in states], axis=1)
        total = acc[head : head + 1]
        levels = three_parts(best + jnp.log(total))
        full = jnp.concatenate(
            [(acc[:head] / total).astype(BF16), *levels, jnp.zeros((PAD - 3, span), BF16)], axis=0
        )
        for n in range(2):
            out[2 * tile + n] = full[:, n * width : (n + 1) * width]

    mixed_tile = lax.div(team, 2)

    def empty_tile(tile, nothing):
        blank = jnp.concatenate(
            [jnp.zeros((head, width), BF16), jnp.full((PAD, width), LOW, BF16)], axis=0
        )
        out[2 * tile] = blank
        out[2 * tile + 1] = blank
        return nothing

    def full_tile(tile, nothing):
        run(tile, count * width // reach, False)
        return nothing

    lax.fori_loop(0, mixed_tile, empty_tile, 0)
    whole = count * width // reach
    steps = jnp.where(lax.rem(team, 2) == 1, lax.div(own * width, reach) + 1, whole)
    run(mixed_tile, steps, True)
    lax.fori_loop(mixed_tile + 1, teams // 2, full_tile, 0)


def partial_attention(place, kv, query, cum):
    teams, head, width = query.shape
    count = kv.shape[0]
    return pl.pallas_call(
        attention_kernel,
        out_shape=jax.ShapeDtypeStruct((teams, head + PAD, width), BF16),
        in_specs=[
            pl.BlockSpec(memory_space=pltpu.SMEM),
            pl.BlockSpec(memory_space=pltpu.VMEM),
            pl.BlockSpec(memory_space=pltpu.VMEM),
            pl.BlockSpec(memory_space=pltpu.VMEM),
        ],
        out_specs=pl.BlockSpec(memory_space=pltpu.VMEM),
        scratch_shapes=[
            pltpu.VMEM((count * width, LANES), BF16),
            pltpu.VMEM((head + PAD, count * width), BF16),
        ],
        compiler_params=pltpu.CompilerParams(vmem_limit_bytes=32 * 1024 * 1024),
        name="partial_attention",
    )(place, kv, query, cum)


def gated_hidden(gate, upward):
    return (jax.nn.silu(gate) * upward).astype(BF16)


def pack_kernel(*refs, shapes):
    sources, target = refs[:-1], refs[-1]
    at = 0
    for source, shape in zip(sources, shapes):
        if len(shape) == 3:
            count, rows, columns = shape
            for e in range(count):
                for k in range(columns // LANES):
                    target[at : at + rows, :] = source[e, :, k * LANES : (k + 1) * LANES]
                    at += rows
        else:
            rows = shape[0]
            target[at : at + rows, :] = source[...]
            at += rows


def packed_shards(*sources):
    shapes = [source.shape for source in sources]
    total = sum(source.size for source in sources) // LANES
    return pl.pallas_call(
        lambda *refs: pack_kernel(*refs, shapes=shapes),
        out_shape=jax.ShapeDtypeStruct((total, LANES), BF16),
        in_specs=[pl.BlockSpec(memory_space=pltpu.VMEM) for _ in sources],
        out_specs=pl.BlockSpec(memory_space=pltpu.VMEM),
        name="pack_shards",
    )(*sources)


def feed_kernel(which, rows, gain, weights, out, gate, upward, down, sems, *, experts):
    shards, hidden = gate.shape[0], gate.shape[1]
    inner = shards * hidden
    features = shards * LANES
    mine = which[0]
    wide = features * hidden // LANES
    bases = [mine * wide, (experts + mine) * wide, 2 * experts * wide + mine * inner]
    for n, target in enumerate((gate, upward)):
        base = pl.multiple_of(bases[n], hidden)
        for k in range(features // LANES):
            pltpu.make_async_copy(
                weights.at[:, pl.ds(base + k * hidden, hidden), :],
                target.at[:, :, pl.ds(k * LANES, LANES)],
                sems.at[n],
            ).start()
    base = pl.multiple_of(bases[2], hidden)
    for t in range(shards):
        pltpu.make_async_copy(
            weights.at[t, pl.ds(base, inner), :], down.at[:, pl.ds(t * LANES, LANES)], sems.at[2]
        ).start()

    floats = [rows[t].astype(F32) for t in range(shards)]
    squares = sum(f * f for f in floats)
    mean = jnp.sum(squares, axis=1, keepdims=True) / features
    inverse = lax.rsqrt(mean + EPS)
    normed = jnp.concatenate([(f * inverse * gain[t]).astype(BF16) for t, f in enumerate(floats)], axis=1)
    across = (((1,), (1,)), ((), ()))
    pltpu.make_async_copy(gate, gate, sems.at[0]).wait()
    first_half = lax.dot_general(
        normed, gate[...].reshape(inner, features), across, preferred_element_type=F32
    )
    pltpu.make_async_copy(upward, upward, sems.at[1]).wait()
    second_half = lax.dot_general(
        normed, upward[...].reshape(inner, features), across, preferred_element_type=F32
    )
    inside = gated_hidden(first_half, second_half)
    pltpu.make_async_copy(down, down, sems.at[2]).wait()
    for t in range(shards):
        part = jnp.dot(inside, down[:, t * LANES : (t + 1) * LANES], preferred_element_type=F32)
        out[t] = part.astype(BF16)


def feed_forward(which, rows, gain, weights, hidden, experts):
    shards = rows.shape[0]
    features = shards * LANES
    inner = shards * hidden
    return pl.pallas_call(
        lambda *refs: feed_kernel(*refs, experts=experts),
        out_shape=jax.ShapeDtypeStruct(rows.shape, BF16),
        in_specs=[
            pl.BlockSpec(memory_space=pltpu.SMEM),
            pl.BlockSpec(memory_space=pltpu.VMEM),
            pl.BlockSpec(memory_space=pltpu.VMEM),
            pl.BlockSpec(memory_space=pltpu.HBM),
        ],
        out_specs=pl.BlockSpec(memory_space=pltpu.VMEM),
        scratch_shapes=[
            pltpu.VMEM((shards, hidden, features), BF16),
            pltpu.VMEM((shards, hidden, features), BF16),
            pltpu.VMEM((inner, features), BF16),
            pltpu.SemaphoreType.DMA((3,)),
        ],
        compiler_params=pltpu.CompilerParams(vmem_limit_bytes=52 * 1024 * 1024),
        name="routed_feed",
    )(which, rows, gain, weights)


def shared_kernel(rows, gain, gate, upward, out):
    shards = rows.shape[0]
    floats = [rows[t].astype(F32) for t in range(shards)]
    squares = sum(f * f for f in floats)
    inverse = lax.rsqrt(jnp.sum(squares, axis=1, keepdims=True) / (shards * LANES) + EPS)
    normed = jnp.concatenate([(f * inverse * gain[t]).astype(BF16) for t, f in enumerate(floats)], axis=1)
    across = (((1,), (1,)), ((), ()))
    out[...] = gated_hidden(
        lax.dot_general(gate[...], normed, across, preferred_element_type=F32),
        lax.dot_general(upward[...], normed, across, preferred_element_type=F32),
    )


def shared_feed(rows, gain, gate, upward):
    return pl.pallas_call(
        shared_kernel,
        out_shape=jax.ShapeDtypeStruct((gate.shape[0], rows.shape[1]), BF16),
        in_specs=[pl.BlockSpec(memory_space=pltpu.VMEM) for _ in range(4)],
        out_specs=pl.BlockSpec(memory_space=pltpu.VMEM),
        compiler_params=pltpu.CompilerParams(vmem_limit_bytes=24 * 1024 * 1024),
        name="shared_feed",
    )(rows, gain, gate, upward)


def per_device(
    queries,
    keys,
    values,
    log_cum,
    residual,
    out_gain,
    w_out,
    ffn_gain,
    routes,
    route_weight,
    sh_gate,
    sh_up,
    sh_down,
    exp_gate,
    exp_up,
    exp_down,
):
    width, head = queries.shape
    near = ("zl", "x")
    whole = ("zh", "zl", "x")
    group = lax.axis_size(near)
    shards = lax.axis_size("tp")
    blocks = lax.axis_size(whole)
    team, own, shard = lax.axis_index("zh"), lax.axis_index(near), lax.axis_index("tp")
    hidden = sh_gate.shape[1]
    local_experts = exp_gate.shape[0]
    owners = shards // local_experts

    scale = head ** (-0.5)
    key_value = jnp.concatenate([keys.T, values.T], axis=0)
    key_value = copy_to_each(key_value, near)
    query = (queries.T.astype(F32) * scale).astype(BF16)
    teams = lax.axis_size("zh")
    moved = [
        lax.ppermute(query, "zh", [(i, (i + n) % teams) for i in range(teams)])
        for n in range(1, teams)
    ]
    query = jnp.stack([query, *moved])
    cum = lax.dynamic_slice_in_dim(log_cum, team * group * width, group * width, 1)
    expert_weights = packed_shards(
        jnp.swapaxes(exp_gate, 1, 2), jnp.swapaxes(exp_up, 1, 2), exp_down.reshape(-1, LANES)
    )
    expert_weights = lax.all_gather(expert_weights, "tp", axis=0, tiled=False)

    place = jnp.stack([team, own]).astype(jnp.int32)
    partial = partial_attention(place, key_value, query, cum)
    partial = exchange(partial, "zh").astype(F32)
    level = partial[:, head] + partial[:, head + 1] + partial[:, head + 2]
    share = jnp.exp(level - jnp.max(level, axis=0, keepdims=True))
    share = share / jnp.sum(share, axis=0, keepdims=True)
    head_out = jnp.sum(partial[:, :head] * share[:, None], axis=0).astype(BF16)

    all_heads = lax.all_gather(head_out[None], "tp", axis=0, tiled=True).astype(F32)
    channels = shards * head
    mean = jnp.sum(all_heads * all_heads, axis=(0, 1), keepdims=True) / channels
    inverse = lax.rsqrt(mean + EPS)
    mixed = (all_heads * inverse * out_gain.reshape(shards, head, 1)).astype(BF16).reshape(channels, width)
    attended = lax.dot_general(mixed, w_out, (((0,), (0,)), ((), ())), preferred_element_type=F32)
    updated = (residual.astype(F32) + attended).astype(BF16)
    all_rows = lax.all_gather(updated[None], "tp", axis=0, tiled=True)

    top = routes.shape[1]
    experts = local_experts * blocks
    capacity = 2 * width * top // experts
    slots = experts * capacity
    chosen = [routes[:, k, None] == lax.iota(jnp.int32, experts)[None, :] for k in range(top)]
    named = sum(c.astype(BF16) for c in chosen)
    earlier = (lax.iota(jnp.int32, width)[:, None] > lax.iota(jnp.int32, width)[None, :]).astype(BF16)
    rank = jnp.dot(earlier, named, preferred_element_type=F32)
    picks = []
    for k in range(top):
        own = jnp.sum(jnp.where(chosen[k], rank, 0.0), axis=1).astype(jnp.int32)
        slot = routes[:, k] * capacity + own
        picks.append(slot[:, None] == lax.iota(jnp.int32, slots)[None, :])
    select = sum(p.astype(BF16) for p in picks)
    weights = sum(jnp.where(p, route_weight[:, k, None], 0.0) for k, p in enumerate(picks))
    weight_high = lax.reduce_precision(weights, 8, 7)
    weight_low = (weights - weight_high).astype(BF16)
    weight_high = weight_high.astype(BF16)
    select, weight_high, weight_low = lax.optimization_barrier((select, weight_high, weight_low))

    outgoing = lax.dot_general(
        select, updated, (((0,), (0,)), ((), ())), preferred_element_type=F32
    ).astype(BF16)
    per_block = local_experts * capacity
    landed = exchange(outgoing.reshape(blocks, per_block, LANES), whole)
    rounds = blocks // owners
    landed = landed.reshape(rounds, owners, local_experts, capacity, LANES)
    landed = jnp.transpose(landed, (2, 1, 0, 3, 4)).reshape(shards, rounds * capacity, LANES)
    rows = exchange(landed, "tp")
    gain = ffn_gain.reshape(shards, 1, LANES)
    mine = (shard // owners).astype(jnp.int32)[None]
    routed_out = feed_forward(mine, rows, gain, expert_weights, hidden, local_experts)
    returned = exchange(routed_out, "tp")
    returned = returned.reshape(local_experts, owners, rounds, capacity, LANES)
    returned = jnp.transpose(returned, (2, 1, 0, 3, 4)).reshape(blocks, per_block, LANES)
    answers = exchange(returned, whole).reshape(slots, LANES)
    share_hidden = shared_feed(all_rows, gain, sh_gate.T, sh_up.T)
    share_hidden = lax.all_gather(share_hidden, "tp", axis=0, tiled=True)
    shared = lax.dot_general(
        share_hidden, sh_down, (((0,), (0,)), ((), ())), preferred_element_type=F32
    )
    routed = jnp.dot(weight_high, answers, preferred_element_type=F32) + jnp.dot(
        weight_low, answers, preferred_element_type=F32
    )
    return (updated.astype(F32) + shared + routed).astype(BF16)


def solution(mesh):
    blocks, shards = mesh.devices.shape
    grid = Mesh(mesh.devices.reshape(*GRIDS[blocks], shards), ("zh", "zl", "x", "tp"))
    sp = ("zh", "zl", "x")
    in_specs = (
        P(sp, "tp"),
        P(sp, "tp"),
        P(sp, "tp"),
        P("tp", None),
        P(sp, "tp"),
        P(),
        P(None, "tp"),
        P(),
        P(sp, None),
        P(sp, None),
        P(None, "tp"),
        P(None, "tp"),
        P(None, "tp"),
        P(sp, None, "tp"),
        P(sp, None, "tp"),
        P(sp, None, "tp"),
    )
    return jax.shard_map(
        per_device, mesh=grid, in_specs=in_specs, out_specs=P(sp, "tp"), check_vma=False
    )
```

```python
import jax
import jax.numpy as jnp
from jax import lax
from jax.experimental import pallas as pl
from jax.experimental.pallas import tpu as pltpu
from jax.sharding import Mesh, PartitionSpec as P


EPS = 1e-06
LANES = 128
LOW = -1e30
PAD = 16
CHAIN = 768
BF16 = jnp.bfloat16
F32 = jnp.float32
GRIDS = {32: (4, 2, 4), 4: (2, 1, 2), 8: (2, 2, 2)}


def exchange(value, axis):
    return lax.all_to_all(value, axis, split_axis=0, concat_axis=0, tiled=True)


def copy_to_each(value, axis):
    return exchange(jnp.broadcast_to(value, (lax.axis_size(axis), *value.shape)), axis)


def three_parts(value):
    high = value.astype(BF16)
    rest = value - high.astype(F32)
    middle = rest.astype(BF16)
    low = (rest - middle.astype(F32)).astype(BF16)
    return [high, middle, low]


def attention_kernel(place, kv, query, cum, out, key_rows, value_rows):
    team, own = place[0], place[1]
    teams, head, width = query.shape
    count = kv.shape[0]
    span = 2 * width
    reach = min(count, 8) * width
    piece = min(span, CHAIN)
    chains = span // piece

    for b in range(count):
        parts = three_parts(-cum[:, b * width : (b + 1) * width])
        filler = jnp.zeros((LANES - head - 3, width), BF16)
        key_rows[b * width : (b + 1) * width] = jnp.concatenate(
            [kv[b, :head, :], *parts, filler], axis=0
        ).T
        value_rows[:, b * width : (b + 1) * width] = jnp.concatenate(
            [kv[b, head:, :], jnp.ones((PAD, width), BF16)], axis=0
        )

    def step(i, part, state, limit):
        best, acc = state
        at = pl.ds(pl.multiple_of(i * reach, reach), reach)
        score = jnp.dot(key_rows[at, :], part, preferred_element_type=F32)
        if limit is not None:
            key_pos = i * reach + lax.broadcasted_iota(jnp.int32, score.shape, 0)
            score = jnp.where(key_pos <= limit, score, LOW)
        new_best = jnp.maximum(best, jnp.max(score, axis=0, keepdims=True))
        weight = jnp.exp(score - new_best).astype(BF16)
        added = jnp.dot(value_rows[:, at], weight, preferred_element_type=F32)
        return new_best, acc * jnp.exp(best - new_best) + added

    def run(tile, steps, masked):
        turns = [lax.rem(team - (2 * tile + n) + teams, teams) for n in range(2)]
        both = jnp.concatenate([query[turn] for turn in turns], axis=1)
        both = jnp.concatenate([both, jnp.ones((LANES - head, span), BF16)], axis=0)
        limits = [None] * chains
        if masked:
            lane = lax.broadcasted_iota(jnp.int32, (1, span), 1)
            block = 2 * tile + jnp.where(lane >= width, 1, 0)
            at = own * width + jnp.where(lane >= width, lane - width, lane)
            limit = jnp.where(block < team, -1, jnp.where(block == team, at, count * width))
            limits = [limit[:, c * piece : (c + 1) * piece] for c in range(chains)]
        parts = [both[:, c * piece : (c + 1) * piece] for c in range(chains)]
        first = tuple(
            (jnp.full((1, piece), LOW, F32), jnp.zeros((head + PAD, piece), F32)) for _ in range(chains)
        )
        states = lax.fori_loop(
            0,
            steps,
            lambda i, s: tuple(step(i, parts[c], s[c], limits[c]) for c in range(chains)),
            first,
        )
        best = jnp.concatenate([m for m, _ in states], axis=1)
        acc = jnp.concatenate([a for _, a in states], axis=1)
        total = acc[head : head + 1]
        levels = three_parts(best + jnp.log(total))
        full = jnp.concatenate(
            [(acc[:head] / total).astype(BF16), *levels, jnp.zeros((PAD - 3, span), BF16)], axis=0
        )
        for n in range(2):
            out[2 * tile + n] = full[:, n * width : (n + 1) * width]

    mixed_tile = lax.div(team, 2)

    def empty_tile(tile, nothing):
        blank = jnp.concatenate(
            [jnp.zeros((head, width), BF16), jnp.full((PAD, width), LOW, BF16)], axis=0
        )
        out[2 * tile] = blank
        out[2 * tile + 1] = blank
        return nothing

    def full_tile(tile, nothing):
        run(tile, count * width // reach, False)
        return nothing

    lax.fori_loop(0, mixed_tile, empty_tile, 0)
    whole = count * width // reach
    steps = jnp.where(lax.rem(team, 2) == 1, lax.div(own * width, reach) + 1, whole)
    run(mixed_tile, steps, True)
    lax.fori_loop(mixed_tile + 1, teams // 2, full_tile, 0)


def partial_attention(place, kv, query, cum):
    teams, head, width = query.shape
    count = kv.shape[0]
    return pl.pallas_call(
        attention_kernel,
        out_shape=jax.ShapeDtypeStruct((teams, head + PAD, width), BF16),
        in_specs=[
            pl.BlockSpec(memory_space=pltpu.SMEM),
            pl.BlockSpec(memory_space=pltpu.VMEM),
            pl.BlockSpec(memory_space=pltpu.VMEM),
            pl.BlockSpec(memory_space=pltpu.VMEM),
        ],
        out_specs=pl.BlockSpec(memory_space=pltpu.VMEM),
        scratch_shapes=[
            pltpu.VMEM((count * width, LANES), BF16),
            pltpu.VMEM((head + PAD, count * width), BF16),
        ],
        compiler_params=pltpu.CompilerParams(vmem_limit_bytes=32 * 1024 * 1024),
        name="partial_attention",
    )(place, kv, query, cum)


def gated_hidden(gate, upward):
    return (jax.nn.silu(gate) * upward).astype(BF16)


def pack_kernel(*refs, shapes):
    sources, target = refs[:-1], refs[-1]
    at = 0
    for source, shape in zip(sources, shapes):
        if len(shape) == 3:
            count, rows, columns = shape
            for e in range(count):
                for k in range(columns // LANES):
                    target[at : at + rows, :] = source[e, :, k * LANES : (k + 1) * LANES]
                    at += rows
        else:
            rows = shape[0]
            target[at : at + rows, :] = source[...]
            at += rows


def packed_shards(*sources):
    shapes = [source.shape for source in sources]
    total = sum(source.size for source in sources) // LANES
    return pl.pallas_call(
        lambda *refs: pack_kernel(*refs, shapes=shapes),
        out_shape=jax.ShapeDtypeStruct((total, LANES), BF16),
        in_specs=[pl.BlockSpec(memory_space=pltpu.VMEM) for _ in sources],
        out_specs=pl.BlockSpec(memory_space=pltpu.VMEM),
        name="pack_shards",
    )(*sources)


def feed_kernel(which, rows, gain, weights, out, gate, upward, *rest, first, count, experts):
    down, sems = rest if len(rest) == 2 else (None, rest[0])
    shards, hidden = gate.shape[0], gate.shape[1]
    inner = shards * hidden
    features = shards * LANES
    mine = which[0]
    wide = features * hidden // LANES
    bases = [mine * wide, (experts + mine) * wide, 2 * experts * wide + mine * inner]
    if down is None:
        shared = experts * (2 * wide + inner)
        bases = [shared, shared + wide, 0]
    for n, target in enumerate((gate, upward)):
        base = bases[n] if down is None else pl.multiple_of(bases[n], hidden)
        for k in range(features // LANES):
            pltpu.make_async_copy(
                weights.at[:, pl.ds(base + k * hidden, hidden), :],
                target.at[:, :, pl.ds(k * LANES, LANES)],
                sems.at[n],
            ).start()
    base = 0 if down is None else pl.multiple_of(bases[2], hidden)
    for t in range(0 if down is None else shards):
        pltpu.make_async_copy(
            weights.at[t, pl.ds(base, inner), :], down.at[:, pl.ds(t * LANES, LANES)], sems.at[2]
        ).start()

    floats = [rows[t, first : first + count].astype(F32) for t in range(shards)]
    squares = sum(f * f for f in floats)
    mean = jnp.sum(squares, axis=1, keepdims=True) / features
    inverse = lax.rsqrt(mean + EPS)
    normed = jnp.concatenate([(f * inverse * gain[t]).astype(BF16) for t, f in enumerate(floats)], axis=1)
    across = (((1,), (1,)), ((), ()))
    pltpu.make_async_copy(gate, gate, sems.at[0]).wait()
    first_half = lax.dot_general(
        normed, gate[...].reshape(inner, features), across, preferred_element_type=F32
    )
    pltpu.make_async_copy(upward, upward, sems.at[1]).wait()
    second_half = lax.dot_general(
        normed, upward[...].reshape(inner, features), across, preferred_element_type=F32
    )
    inside = gated_hidden(first_half, second_half)
    if down is None:
        out[...] = inside
        return
    pltpu.make_async_copy(down, down, sems.at[2]).wait()
    for t in range(shards):
        part = jnp.dot(inside, down[:, t * LANES : (t + 1) * LANES], preferred_element_type=F32)
        out[t] = part.astype(BF16)


def feed_forward(which, rows, gain, weights, hidden, experts, first, count, whole):
    shards = rows.shape[0]
    features = shards * LANES
    inner = shards * hidden
    shape = (shards, count, LANES) if whole else (count, inner)
    down = [pltpu.VMEM((inner, features), BF16)] if whole else []
    return pl.pallas_call(
        lambda *refs: feed_kernel(*refs, first=first, count=count, experts=experts),
        out_shape=jax.ShapeDtypeStruct(shape, BF16),
        in_specs=[
            pl.BlockSpec(memory_space=pltpu.SMEM),
            pl.BlockSpec(memory_space=pltpu.VMEM),
            pl.BlockSpec(memory_space=pltpu.VMEM),
            pl.BlockSpec(memory_space=pltpu.HBM),
        ],
        out_specs=pl.BlockSpec(memory_space=pltpu.VMEM),
        scratch_shapes=[
            pltpu.VMEM((shards, hidden, features), BF16),
            pltpu.VMEM((shards, hidden, features), BF16),
            *down,
            pltpu.SemaphoreType.DMA((3,)),
        ],
        compiler_params=pltpu.CompilerParams(vmem_limit_bytes=52 * 1024 * 1024),
        name="routed_feed" if whole else "shared_feed",
    )(which, rows, gain, weights)


def per_device(
    queries,
    keys,
    values,
    log_cum,
    residual,
    out_gain,
    w_out,
    ffn_gain,
    routes,
    route_weight,
    sh_gate,
    sh_up,
    sh_down,
    exp_gate,
    exp_up,
    exp_down,
):
    width, head = queries.shape
    near = ("zl", "x")
    whole = ("zh", "zl", "x")
    group = lax.axis_size(near)
    shards = lax.axis_size("tp")
    blocks = lax.axis_size(whole)
    team, own, shard = lax.axis_index("zh"), lax.axis_index(near), lax.axis_index("tp")
    hidden = sh_gate.shape[1]
    local_experts = exp_gate.shape[0]
    owners = shards // local_experts

    scale = head ** (-0.5)
    key_value = jnp.concatenate([keys.T, values.T], axis=0)
    key_value = copy_to_each(key_value, near)
    query = (queries.T.astype(F32) * scale).astype(BF16)
    teams = lax.axis_size("zh")
    moved = [
        lax.ppermute(query, "zh", [(i, (i + n) % teams) for i in range(teams)])
        for n in range(1, teams)
    ]
    query = jnp.stack([query, *moved])
    cum = lax.dynamic_slice_in_dim(log_cum, team * group * width, group * width, 1)
    expert_weights = packed_shards(
        jnp.swapaxes(exp_gate, 1, 2),
        jnp.swapaxes(exp_up, 1, 2),
        exp_down.reshape(-1, LANES),
        sh_gate.T[None],
        sh_up.T[None],
    )
    expert_weights = lax.all_gather(expert_weights, "tp", axis=0, tiled=False)

    place = jnp.stack([team, own]).astype(jnp.int32)
    partial = partial_attention(place, key_value, query, cum)
    partial = exchange(partial, "zh").astype(F32)
    level = partial[:, head] + partial[:, head + 1] + partial[:, head + 2]
    share = jnp.exp(level - jnp.max(level, axis=0, keepdims=True))
    share = share / jnp.sum(share, axis=0, keepdims=True)
    head_out = jnp.sum(partial[:, :head] * share[:, None], axis=0).astype(BF16)

    all_heads = lax.all_gather(head_out[None], "tp", axis=0, tiled=True).astype(F32)
    channels = shards * head
    mean = jnp.sum(all_heads * all_heads, axis=(0, 1), keepdims=True) / channels
    inverse = lax.rsqrt(mean + EPS)
    mixed = (all_heads * inverse * out_gain.reshape(shards, head, 1)).astype(BF16).reshape(channels, width)
    attended = lax.dot_general(mixed, w_out, (((0,), (0,)), ((), ())), preferred_element_type=F32)
    updated = (residual.astype(F32) + attended).astype(BF16)

    top = routes.shape[1]
    experts = local_experts * blocks
    capacity = 2 * width * top // experts
    slots = experts * capacity
    chosen = [routes[:, k, None] == lax.iota(jnp.int32, experts)[None, :] for k in range(top)]
    named = sum(c.astype(BF16) for c in chosen)
    earlier = (lax.iota(jnp.int32, width)[:, None] > lax.iota(jnp.int32, width)[None, :]).astype(BF16)
    rank = jnp.dot(earlier, named, preferred_element_type=F32)
    picks, turned = [], []
    for k in range(top):
        own = jnp.sum(jnp.where(chosen[k], rank, 0.0), axis=1).astype(jnp.int32)
        slot = routes[:, k] * capacity + own
        picks.append(slot[:, None] == lax.iota(jnp.int32, slots)[None, :])
        turned.append(lax.iota(jnp.int32, slots)[:, None] == slot[None, :])
    select = sum(t.astype(BF16) for t in turned)
    weights = sum(jnp.where(p, route_weight[:, k, None], 0.0) for k, p in enumerate(picks))
    weight_high = lax.reduce_precision(weights, 8, 7)
    weight_low = (weights - weight_high).astype(BF16)
    weight_high = weight_high.astype(BF16)
    select, weight_high, weight_low = lax.optimization_barrier((select, weight_high, weight_low))

    outgoing = jnp.dot(select, updated, preferred_element_type=F32).astype(BF16)
    per_block = local_experts * capacity
    landed = exchange(outgoing.reshape(blocks, per_block, LANES), whole)
    rounds = blocks // owners
    landed = landed.reshape(rounds, owners, local_experts, capacity, LANES)
    landed = jnp.transpose(landed, (2, 1, 0, 3, 4)).reshape(shards, rounds * capacity, LANES)
    own_rows = updated.reshape(shards, width // shards, LANES)
    rows = exchange(jnp.concatenate([landed, own_rows], axis=1), "tp")
    gain = ffn_gain.reshape(shards, 1, LANES)
    mine = (shard // owners).astype(jnp.int32)[None]
    routed_rows = rounds * capacity
    routed_out = feed_forward(
        mine, rows, gain, expert_weights, hidden, local_experts, 0, routed_rows, True
    )
    returned = exchange(routed_out, "tp")
    returned = returned.reshape(local_experts, owners, rounds, capacity, LANES)
    returned = jnp.transpose(returned, (2, 1, 0, 3, 4)).reshape(blocks, per_block, LANES)
    answers = exchange(returned, whole).reshape(slots, LANES)
    share_hidden = feed_forward(
        mine, rows, gain, expert_weights, hidden, local_experts, routed_rows, width // shards, False
    )
    share_hidden = lax.all_gather(share_hidden, "tp", axis=0, tiled=True)
    shared = jnp.dot(share_hidden, sh_down, preferred_element_type=F32)
    routed = jnp.dot(weight_high, answers, preferred_element_type=F32) + jnp.dot(
        weight_low, answers, preferred_element_type=F32
    )
    return (updated.astype(F32) + shared + routed).astype(BF16)


def solution(mesh):
    blocks, shards = mesh.devices.shape
    grid = Mesh(mesh.devices.reshape(*GRIDS[blocks], shards), ("zh", "zl", "x", "tp"))
    sp = ("zh", "zl", "x")
    in_specs = (
        P(sp, "tp"),
        P(sp, "tp"),
        P(sp, "tp"),
        P("tp", None),
        P(sp, "tp"),
        P(),
        P(None, "tp"),
        P(),
        P(sp, None),
        P(sp, None),
        P(None, "tp"),
        P(None, "tp"),
        P(None, "tp"),
        P(sp, None, "tp"),
        P(sp, None, "tp"),
        P(sp, None, "tp"),
    )
    return jax.shard_map(
        per_device, mesh=grid, in_specs=in_specs, out_specs=P(sp, "tp"), check_vma=False
    )
```

```python
import jax
import jax.numpy as jnp
from jax import lax
from jax.experimental import pallas as pl
from jax.experimental.pallas import tpu as pltpu
from jax.sharding import Mesh, PartitionSpec as P


EPS = 1e-06
LANES = 128
LOW = -1e30
PAD = 16
CHAIN = 768
BF16 = jnp.bfloat16
F32 = jnp.float32
GRIDS = {32: (4, 2, 4), 4: (2, 1, 2), 8: (2, 2, 2)}


def exchange(value, axis):
    return lax.all_to_all(value, axis, split_axis=0, concat_axis=0, tiled=True)


def copy_to_each(value, axis):
    return exchange(jnp.broadcast_to(value, (lax.axis_size(axis), *value.shape)), axis)


def three_parts(value):
    high = value.astype(BF16)
    rest = value - high.astype(F32)
    middle = rest.astype(BF16)
    low = (rest - middle.astype(F32)).astype(BF16)
    return [high, middle, low]


def attention_kernel(place, kv, query, cum, out, key_rows, value_rows):
    team, own = place[0], place[1]
    teams, head, width = query.shape
    count = kv.shape[0]
    span = 2 * width
    reach = min(count, 8) * width
    piece = min(span, CHAIN)
    chains = span // piece

    for b in range(count):
        parts = three_parts(-cum[:, b * width : (b + 1) * width])
        filler = jnp.zeros((LANES - head - 3, width), BF16)
        key_rows[b * width : (b + 1) * width] = jnp.concatenate(
            [kv[b, :head, :], *parts, filler], axis=0
        ).T
        value_rows[:, b * width : (b + 1) * width] = jnp.concatenate(
            [kv[b, head:, :], jnp.ones((PAD, width), BF16)], axis=0
        )

    def step(i, part, state, limit):
        best, acc = state
        at = pl.ds(pl.multiple_of(i * reach, reach), reach)
        score = jnp.dot(key_rows[at, :], part, preferred_element_type=F32)
        if limit is not None:
            key_pos = i * reach + lax.broadcasted_iota(jnp.int32, score.shape, 0)
            score = jnp.where(key_pos <= limit, score, LOW)
        new_best = jnp.maximum(best, jnp.max(score, axis=0, keepdims=True))
        weight = jnp.exp(score - new_best).astype(BF16)
        added = jnp.dot(value_rows[:, at], weight, preferred_element_type=F32)
        return new_best, acc * jnp.exp(best - new_best) + added

    def run(tile, steps, masked):
        turns = [lax.rem(team - (2 * tile + n) + teams, teams) for n in range(2)]
        both = jnp.concatenate([query[turn] for turn in turns], axis=1)
        both = jnp.concatenate([both, jnp.ones((LANES - head, span), BF16)], axis=0)
        limits = [None] * chains
        if masked:
            lane = lax.broadcasted_iota(jnp.int32, (1, span), 1)
            block = 2 * tile + jnp.where(lane >= width, 1, 0)
            at = own * width + jnp.where(lane >= width, lane - width, lane)
            limit = jnp.where(block < team, -1, jnp.where(block == team, at, count * width))
            limits = [limit[:, c * piece : (c + 1) * piece] for c in range(chains)]
        parts = [both[:, c * piece : (c + 1) * piece] for c in range(chains)]
        first = tuple(
            (jnp.full((1, piece), LOW, F32), jnp.zeros((head + PAD, piece), F32)) for _ in range(chains)
        )
        states = lax.fori_loop(
            0,
            steps,
            lambda i, s: tuple(step(i, parts[c], s[c], limits[c]) for c in range(chains)),
            first,
        )
        best = jnp.concatenate([m for m, _ in states], axis=1)
        acc = jnp.concatenate([a for _, a in states], axis=1)
        total = acc[head : head + 1]
        levels = three_parts(best + jnp.log(total))
        full = jnp.concatenate(
            [(acc[:head] / total).astype(BF16), *levels, jnp.zeros((PAD - 3, span), BF16)], axis=0
        )
        for n in range(2):
            out[2 * tile + n] = full[:, n * width : (n + 1) * width]

    mixed_tile = lax.div(team, 2)

    def empty_tile(tile, nothing):
        blank = jnp.concatenate(
            [jnp.zeros((head, width), BF16), jnp.full((PAD, width), LOW, BF16)], axis=0
        )
        out[2 * tile] = blank
        out[2 * tile + 1] = blank
        return nothing

    def full_tile(tile, nothing):
        run(tile, count * width // reach, False)
        return nothing

    lax.fori_loop(0, mixed_tile, empty_tile, 0)
    whole = count * width // reach
    steps = jnp.where(lax.rem(team, 2) == 1, lax.div(own * width, reach) + 1, whole)
    run(mixed_tile, steps, True)
    lax.fori_loop(mixed_tile + 1, teams // 2, full_tile, 0)


def partial_attention(place, kv, query, cum):
    teams, head, width = query.shape
    count = kv.shape[0]
    return pl.pallas_call(
        attention_kernel,
        out_shape=jax.ShapeDtypeStruct((teams, head + PAD, width), BF16),
        in_specs=[
            pl.BlockSpec(memory_space=pltpu.SMEM),
            pl.BlockSpec(memory_space=pltpu.VMEM),
            pl.BlockSpec(memory_space=pltpu.VMEM),
            pl.BlockSpec(memory_space=pltpu.VMEM),
        ],
        out_specs=pl.BlockSpec(memory_space=pltpu.VMEM),
        scratch_shapes=[
            pltpu.VMEM((count * width, LANES), BF16),
            pltpu.VMEM((head + PAD, count * width), BF16),
        ],
        compiler_params=pltpu.CompilerParams(vmem_limit_bytes=32 * 1024 * 1024),
        name="partial_attention",
    )(place, kv, query, cum)


def gated_hidden(gate, upward):
    return (jax.nn.silu(gate) * upward).astype(BF16)


def pack_kernel(*refs, shapes):
    sources, target = refs[:-1], refs[-1]
    at = 0
    for source, shape in zip(sources, shapes):
        if len(shape) == 3:
            count, rows, columns = shape
            for e in range(count):
                for k in range(columns // LANES):
                    target[at : at + rows, :] = source[e, :, k * LANES : (k + 1) * LANES]
                    at += rows
        else:
            rows = shape[0]
            target[at : at + rows, :] = source[...]
            at += rows


def packed_shards(*sources):
    shapes = [source.shape for source in sources]
    total = sum(source.size for source in sources) // LANES
    return pl.pallas_call(
        lambda *refs: pack_kernel(*refs, shapes=shapes),
        out_shape=jax.ShapeDtypeStruct((total, LANES), BF16),
        in_specs=[pl.BlockSpec(memory_space=pltpu.VMEM) for _ in sources],
        out_specs=pl.BlockSpec(memory_space=pltpu.VMEM),
        name="pack_shards",
    )(*sources)


def feed_kernel(which, rows, gain, weights, out, gate, upward, down, sems, *, experts):
    shards, hidden = gate.shape[0], gate.shape[1]
    inner = shards * hidden
    features = shards * LANES
    mine = which[0]
    wide = features * hidden // LANES
    bases = [mine * wide, (experts + mine) * wide, 2 * experts * wide + mine * inner]
    for n, target in enumerate((gate, upward)):
        base = pl.multiple_of(bases[n], hidden)
        for k in range(features // LANES):
            pltpu.make_async_copy(
                weights.at[:, pl.ds(base + k * hidden, hidden), :],
                target.at[:, :, pl.ds(k * LANES, LANES)],
                sems.at[n],
            ).start()
    base = pl.multiple_of(bases[2], hidden)
    for t in range(shards):
        pltpu.make_async_copy(
            weights.at[t, pl.ds(base, inner), :], down.at[:, pl.ds(t * LANES, LANES)], sems.at[2]
        ).start()

    floats = [rows[t].astype(F32) for t in range(shards)]
    squares = sum(f * f for f in floats)
    mean = jnp.sum(squares, axis=1, keepdims=True) / features
    inverse = lax.rsqrt(mean + EPS)
    normed = jnp.concatenate([(f * inverse * gain[t]).astype(BF16) for t, f in enumerate(floats)], axis=1)
    across = (((1,), (1,)), ((), ()))
    pltpu.make_async_copy(gate, gate, sems.at[0]).wait()
    first_half = lax.dot_general(
        normed, gate[...].reshape(inner, features), across, preferred_element_type=F32
    )
    pltpu.make_async_copy(upward, upward, sems.at[1]).wait()
    second_half = lax.dot_general(
        normed, upward[...].reshape(inner, features), across, preferred_element_type=F32
    )
    inside = gated_hidden(first_half, second_half)
    pltpu.make_async_copy(down, down, sems.at[2]).wait()
    for t in range(shards):
        part = jnp.dot(inside, down[:, t * LANES : (t + 1) * LANES], preferred_element_type=F32)
        out[t] = part.astype(BF16)


def feed_forward(which, rows, gain, weights, hidden, experts):
    shards = rows.shape[0]
    features = shards * LANES
    inner = shards * hidden
    return pl.pallas_call(
        lambda *refs: feed_kernel(*refs, experts=experts),
        out_shape=jax.ShapeDtypeStruct(rows.shape, BF16),
        in_specs=[
            pl.BlockSpec(memory_space=pltpu.SMEM),
            pl.BlockSpec(memory_space=pltpu.VMEM),
            pl.BlockSpec(memory_space=pltpu.VMEM),
            pl.BlockSpec(memory_space=pltpu.HBM),
        ],
        out_specs=pl.BlockSpec(memory_space=pltpu.VMEM),
        scratch_shapes=[
            pltpu.VMEM((shards, hidden, features), BF16),
            pltpu.VMEM((shards, hidden, features), BF16),
            pltpu.VMEM((inner, features), BF16),
            pltpu.SemaphoreType.DMA((3,)),
        ],
        compiler_params=pltpu.CompilerParams(vmem_limit_bytes=52 * 1024 * 1024),
        name="routed_feed",
    )(which, rows, gain, weights)


def shared_kernel(rows, gain, gate, upward, out):
    shards = rows.shape[0]
    floats = [rows[t].astype(F32) for t in range(shards)]
    squares = sum(f * f for f in floats)
    inverse = lax.rsqrt(jnp.sum(squares, axis=1, keepdims=True) / (shards * LANES) + EPS)
    normed = jnp.concatenate([(f * inverse * gain[t]).astype(BF16) for t, f in enumerate(floats)], axis=1)
    across = (((1,), (1,)), ((), ()))
    out[...] = gated_hidden(
        lax.dot_general(gate[...], normed, across, preferred_element_type=F32),
        lax.dot_general(upward[...], normed, across, preferred_element_type=F32),
    )


def shared_feed(rows, gain, gate, upward):
    return pl.pallas_call(
        shared_kernel,
        out_shape=jax.ShapeDtypeStruct((gate.shape[0], rows.shape[1]), BF16),
        in_specs=[pl.BlockSpec(memory_space=pltpu.VMEM) for _ in range(4)],
        out_specs=pl.BlockSpec(memory_space=pltpu.VMEM),
        compiler_params=pltpu.CompilerParams(vmem_limit_bytes=24 * 1024 * 1024),
        name="shared_feed",
    )(rows, gain, gate, upward)


def per_device(
    queries,
    keys,
    values,
    log_cum,
    residual,
    out_gain,
    w_out,
    ffn_gain,
    routes,
    route_weight,
    sh_gate,
    sh_up,
    sh_down,
    exp_gate,
    exp_up,
    exp_down,
):
    width, head = queries.shape
    near = ("zl", "x")
    whole = ("zh", "zl", "x")
    group = lax.axis_size(near)
    shards = lax.axis_size("tp")
    blocks = lax.axis_size(whole)
    team, own, shard = lax.axis_index("zh"), lax.axis_index(near), lax.axis_index("tp")
    hidden = sh_gate.shape[1]
    local_experts = exp_gate.shape[0]
    owners = shards // local_experts

    scale = head ** (-0.5)
    key_value = jnp.concatenate([keys.T, values.T], axis=0)
    key_value = copy_to_each(key_value, near)
    query = (queries.T.astype(F32) * scale).astype(BF16)
    teams = lax.axis_size("zh")
    moved = [
        lax.ppermute(query, "zh", [(i, (i + n) % teams) for i in range(teams)])
        for n in range(1, teams)
    ]
    query = jnp.stack([query, *moved])
    cum = lax.dynamic_slice_in_dim(log_cum, team * group * width, group * width, 1)
    expert_weights = packed_shards(
        jnp.swapaxes(exp_gate, 1, 2), jnp.swapaxes(exp_up, 1, 2), exp_down.reshape(-1, LANES)
    )
    expert_weights = lax.all_gather(expert_weights, "tp", axis=0, tiled=False)

    place = jnp.stack([team, own]).astype(jnp.int32)
    partial = partial_attention(place, key_value, query, cum)
    partial = exchange(partial, "zh")
    partial = partial.astype(F32)
    level = partial[:, head] + partial[:, head + 1] + partial[:, head + 2]
    share = jnp.exp(level - jnp.max(level, axis=0, keepdims=True))
    share = share / jnp.sum(share, axis=0, keepdims=True)
    head_out = jnp.sum(partial[:, :head] * share[:, None], axis=0).astype(BF16)

    all_heads = lax.all_gather(head_out[None], "tp", axis=0, tiled=True).astype(F32)
    channels = shards * head
    mean = jnp.sum(all_heads * all_heads, axis=(0, 1), keepdims=True) / channels
    inverse = lax.rsqrt(mean + EPS)
    mixed = (all_heads * inverse * out_gain.reshape(shards, head, 1)).astype(BF16).reshape(channels, width)
    attended = lax.dot_general(mixed, w_out, (((0,), (0,)), ((), ())), preferred_element_type=F32)
    updated = (residual.astype(F32) + attended).astype(BF16)
    all_rows = lax.all_gather(updated[None], "tp", axis=0, tiled=True)

    top = routes.shape[1]
    experts = local_experts * blocks
    capacity = 2 * width * top // experts
    slots = experts * capacity
    chosen = [routes[:, k, None] == lax.iota(jnp.int32, experts)[None, :] for k in range(top)]
    named = sum(c.astype(BF16) for c in chosen)
    earlier = (lax.iota(jnp.int32, width)[:, None] > lax.iota(jnp.int32, width)[None, :]).astype(BF16)
    rank = jnp.dot(earlier, named, preferred_element_type=F32)
    picks, turned = [], []
    for k in range(top):
        own = jnp.sum(jnp.where(chosen[k], rank, 0.0), axis=1).astype(jnp.int32)
        slot = routes[:, k] * capacity + own
        picks.append(slot[:, None] == lax.iota(jnp.int32, slots)[None, :])
        turned.append(lax.iota(jnp.int32, slots)[:, None] == slot[None, :])
    select = lax.optimization_barrier(sum(t.astype(BF16) for t in turned))
    weights = sum(jnp.where(p, route_weight[:, k, None], 0.0) for k, p in enumerate(picks))
    weight_high = lax.reduce_precision(weights, 8, 7)
    weight_low = (weights - weight_high).astype(BF16)
    weight_high = weight_high.astype(BF16)
    weight_high, weight_low = lax.optimization_barrier((weight_high, weight_low))

    outgoing = jnp.dot(select, updated, preferred_element_type=F32).astype(BF16)
    per_block = local_experts * capacity
    landed = exchange(outgoing.reshape(blocks, per_block, LANES), whole)
    rounds = blocks // owners
    landed = landed.reshape(rounds, owners, local_experts, capacity, LANES)
    landed = jnp.transpose(landed, (2, 1, 0, 3, 4)).reshape(shards, rounds * capacity, LANES)
    rows = exchange(landed, "tp")
    gain = ffn_gain.reshape(shards, 1, LANES)
    mine = (shard // owners).astype(jnp.int32)[None]
    routed_out = feed_forward(mine, rows, gain, expert_weights, hidden, local_experts)
    returned = exchange(routed_out, "tp")
    returned = returned.reshape(local_experts, owners, rounds, capacity, LANES)
    returned = jnp.transpose(returned, (2, 1, 0, 3, 4)).reshape(blocks, per_block, LANES)
    answers = exchange(returned, whole).reshape(slots, LANES)
    share_hidden = shared_feed(all_rows, gain, sh_gate.T, sh_up.T)
    share_hidden = lax.all_gather(share_hidden, "tp", axis=0, tiled=True)
    shared = lax.dot_general(
        share_hidden, sh_down, (((0,), (0,)), ((), ())), preferred_element_type=F32
    )
    routed = jnp.dot(weight_high, answers, preferred_element_type=F32) + jnp.dot(
        weight_low, answers, preferred_element_type=F32
    )
    return (updated.astype(F32) + shared + routed).astype(BF16)


def solution(mesh):
    blocks, shards = mesh.devices.shape
    grid = Mesh(mesh.devices.reshape(*GRIDS[blocks], shards), ("zh", "zl", "x", "tp"))
    sp = ("zh", "zl", "x")
    in_specs = (
        P(sp, "tp"),
        P(sp, "tp"),
        P(sp, "tp"),
        P("tp", None),
        P(sp, "tp"),
        P(),
        P(None, "tp"),
        P(),
        P(sp, None),
        P(sp, None),
        P(None, "tp"),
        P(None, "tp"),
        P(None, "tp"),
        P(sp, None, "tp"),
        P(sp, None, "tp"),
        P(sp, None, "tp"),
    )
    return jax.shard_map(
        per_device, mesh=grid, in_specs=in_specs, out_specs=P(sp, "tp"), check_vma=False
    )
```

```python
import jax
import jax.numpy as jnp
from jax import lax
from jax.experimental import pallas as pl
from jax.experimental.pallas import tpu as pltpu
from jax.sharding import Mesh, PartitionSpec as P


EPS = 1e-06
LANES = 128
LOW = -1e30
PAD = 16
CHAIN = 768
BF16 = jnp.bfloat16
F32 = jnp.float32
GRIDS = {32: (4, 2, 4), 4: (2, 1, 2), 8: (2, 2, 2)}


def exchange(value, axis):
    return lax.all_to_all(value, axis, split_axis=0, concat_axis=0, tiled=True)


def three_parts(value):
    high = value.astype(BF16)
    rest = value - high.astype(F32)
    middle = rest.astype(BF16)
    low = (rest - middle.astype(F32)).astype(BF16)
    return [high, middle, low]


def attention_kernel(place, kv, query, cum, out, key_rows, value_rows):
    team, own = place[0], place[1]
    teams, head, width = query.shape
    count = kv.shape[0]
    span = 2 * width
    reach = min(count, 8) * width
    piece = min(span, CHAIN)
    chains = span // piece

    for b in range(count):
        parts = three_parts(-cum[:, b * width : (b + 1) * width])
        filler = jnp.zeros((LANES - head - 3, width), BF16)
        key_rows[b * width : (b + 1) * width] = jnp.concatenate(
            [kv[b, :head, :], *parts, filler], axis=0
        ).T
        value_rows[:, b * width : (b + 1) * width] = jnp.concatenate(
            [kv[b, head:, :], jnp.ones((PAD, width), BF16)], axis=0
        )

    def step(i, part, state, limit):
        best, acc = state
        at = pl.ds(pl.multiple_of(i * reach, reach), reach)
        score = jnp.dot(key_rows[at, :], part, preferred_element_type=F32)
        if limit is not None:
            key_pos = i * reach + lax.broadcasted_iota(jnp.int32, score.shape, 0)
            score = jnp.where(key_pos <= limit, score, LOW)
        new_best = jnp.maximum(best, jnp.max(score, axis=0, keepdims=True))
        weight = jnp.exp(score - new_best).astype(BF16)
        added = jnp.dot(value_rows[:, at], weight, preferred_element_type=F32)
        return new_best, acc * jnp.exp(best - new_best) + added

    def run(tile, steps, masked):
        turns = [lax.rem(team - (2 * tile + n) + teams, teams) for n in range(2)]
        both = jnp.concatenate([query[turn] for turn in turns], axis=1)
        both = jnp.concatenate([both, jnp.ones((LANES - head, span), BF16)], axis=0)
        limits = [None] * chains
        if masked:
            lane = lax.broadcasted_iota(jnp.int32, (1, span), 1)
            block = 2 * tile + jnp.where(lane >= width, 1, 0)
            at = own * width + jnp.where(lane >= width, lane - width, lane)
            limit = jnp.where(block < team, -1, jnp.where(block == team, at, count * width))
            limits = [limit[:, c * piece : (c + 1) * piece] for c in range(chains)]
        parts = [both[:, c * piece : (c + 1) * piece] for c in range(chains)]
        first = tuple(
            (jnp.full((1, piece), LOW, F32), jnp.zeros((head + PAD, piece), F32)) for _ in range(chains)
        )
        states = lax.fori_loop(
            0,
            steps,
            lambda i, s: tuple(step(i, parts[c], s[c], limits[c]) for c in range(chains)),
            first,
        )
        best = jnp.concatenate([m for m, _ in states], axis=1)
        acc = jnp.concatenate([a for _, a in states], axis=1)
        total = acc[head : head + 1]
        levels = three_parts(best + jnp.log(total))
        full = jnp.concatenate(
            [(acc[:head] / total).astype(BF16), *levels, jnp.zeros((PAD - 3, span), BF16)], axis=0
        )
        for n in range(2):
            out[2 * tile + n] = full[:, n * width : (n + 1) * width]

    mixed_tile = lax.div(team, 2)

    def empty_tile(tile, nothing):
        blank = jnp.concatenate(
            [jnp.zeros((head, width), BF16), jnp.full((PAD, width), LOW, BF16)], axis=0
        )
        out[2 * tile] = blank
        out[2 * tile + 1] = blank
        return nothing

    def full_tile(tile, nothing):
        run(tile, count * width // reach, False)
        return nothing

    lax.fori_loop(0, mixed_tile, empty_tile, 0)
    whole = count * width // reach
    steps = jnp.where(lax.rem(team, 2) == 1, lax.div(own * width, reach) + 1, whole)
    run(mixed_tile, steps, True)
    lax.fori_loop(mixed_tile + 1, teams // 2, full_tile, 0)


def partial_attention(place, kv, query, cum):
    teams, head, width = query.shape
    count = kv.shape[0]
    return pl.pallas_call(
        attention_kernel,
        out_shape=jax.ShapeDtypeStruct((teams, head + PAD, width), BF16),
        in_specs=[
            pl.BlockSpec(memory_space=pltpu.SMEM),
            pl.BlockSpec(memory_space=pltpu.VMEM),
            pl.BlockSpec(memory_space=pltpu.VMEM),
            pl.BlockSpec(memory_space=pltpu.VMEM),
        ],
        out_specs=pl.BlockSpec(memory_space=pltpu.VMEM),
        scratch_shapes=[
            pltpu.VMEM((count * width, LANES), BF16),
            pltpu.VMEM((head + PAD, count * width), BF16),
        ],
        compiler_params=pltpu.CompilerParams(vmem_limit_bytes=32 * 1024 * 1024),
        name="partial_attention",
    )(place, kv, query, cum)


def gated_hidden(gate, upward):
    return (jax.nn.silu(gate) * upward).astype(BF16)


def pack_kernel(*refs, shapes):
    sources, target = refs[:-1], refs[-1]
    at = 0
    for source, shape in zip(sources, shapes):
        if len(shape) == 3:
            count, rows, columns = shape
            for e in range(count):
                for k in range(columns // LANES):
                    target[at : at + rows, :] = source[e, :, k * LANES : (k + 1) * LANES]
                    at += rows
        else:
            rows = shape[0]
            target[at : at + rows, :] = source[...]
            at += rows


def packed_shards(*sources):
    shapes = [source.shape for source in sources]
    total = sum(source.size for source in sources) // LANES
    return pl.pallas_call(
        lambda *refs: pack_kernel(*refs, shapes=shapes),
        out_shape=jax.ShapeDtypeStruct((total, LANES), BF16),
        in_specs=[pl.BlockSpec(memory_space=pltpu.VMEM) for _ in sources],
        out_specs=pl.BlockSpec(memory_space=pltpu.VMEM),
        name="pack_shards",
    )(*sources)


def feed_kernel(which, rows, gain, weights, out, gate, upward, down, sems, *, experts):
    shards, hidden = gate.shape[0], gate.shape[1]
    inner = shards * hidden
    features = shards * LANES
    mine = which[0]
    wide = features * hidden // LANES
    bases = [mine * wide, (experts + mine) * wide, 2 * experts * wide + mine * inner]
    for n, target in enumerate((gate, upward)):
        base = pl.multiple_of(bases[n], hidden)
        for k in range(features // LANES):
            pltpu.make_async_copy(
                weights.at[:, pl.ds(base + k * hidden, hidden), :],
                target.at[:, :, pl.ds(k * LANES, LANES)],
                sems.at[n],
            ).start()
    base = pl.multiple_of(bases[2], hidden)
    for t in range(shards):
        pltpu.make_async_copy(
            weights.at[t, pl.ds(base, inner), :], down.at[:, pl.ds(t * LANES, LANES)], sems.at[2]
        ).start()

    floats = [rows[t].astype(F32) for t in range(shards)]
    squares = sum(f * f for f in floats)
    mean = jnp.sum(squares, axis=1, keepdims=True) / features
    inverse = lax.rsqrt(mean + EPS)
    normed = jnp.concatenate([(f * inverse * gain[t]).astype(BF16) for t, f in enumerate(floats)], axis=1)
    across = (((1,), (1,)), ((), ()))
    pltpu.make_async_copy(gate, gate, sems.at[0]).wait()
    first_half = lax.dot_general(
        normed, gate[...].reshape(inner, features), across, preferred_element_type=F32
    )
    pltpu.make_async_copy(upward, upward, sems.at[1]).wait()
    second_half = lax.dot_general(
        normed, upward[...].reshape(inner, features), across, preferred_element_type=F32
    )
    inside = gated_hidden(first_half, second_half)
    pltpu.make_async_copy(down, down, sems.at[2]).wait()
    for t in range(shards):
        part = jnp.dot(inside, down[:, t * LANES : (t + 1) * LANES], preferred_element_type=F32)
        out[t] = part.astype(BF16)


def feed_forward(which, rows, gain, weights, hidden, experts):
    shards = rows.shape[0]
    features = shards * LANES
    inner = shards * hidden
    return pl.pallas_call(
        lambda *refs: feed_kernel(*refs, experts=experts),
        out_shape=jax.ShapeDtypeStruct(rows.shape, BF16),
        in_specs=[
            pl.BlockSpec(memory_space=pltpu.SMEM),
            pl.BlockSpec(memory_space=pltpu.VMEM),
            pl.BlockSpec(memory_space=pltpu.VMEM),
            pl.BlockSpec(memory_space=pltpu.HBM),
        ],
        out_specs=pl.BlockSpec(memory_space=pltpu.VMEM),
        scratch_shapes=[
            pltpu.VMEM((shards, hidden, features), BF16),
            pltpu.VMEM((shards, hidden, features), BF16),
            pltpu.VMEM((inner, features), BF16),
            pltpu.SemaphoreType.DMA((3,)),
        ],
        compiler_params=pltpu.CompilerParams(vmem_limit_bytes=52 * 1024 * 1024),
        name="routed_feed",
    )(which, rows, gain, weights)


def shared_kernel(rows, gain, gate, upward, out):
    shards = rows.shape[0]
    floats = [rows[t].astype(F32) for t in range(shards)]
    squares = sum(f * f for f in floats)
    inverse = lax.rsqrt(jnp.sum(squares, axis=1, keepdims=True) / (shards * LANES) + EPS)
    normed = jnp.concatenate([(f * inverse * gain[t]).astype(BF16) for t, f in enumerate(floats)], axis=1)
    across = (((1,), (1,)), ((), ()))
    out[...] = gated_hidden(
        lax.dot_general(gate[...], normed, across, preferred_element_type=F32),
        lax.dot_general(upward[...], normed, across, preferred_element_type=F32),
    )


def shared_feed(rows, gain, gate, upward):
    return pl.pallas_call(
        shared_kernel,
        out_shape=jax.ShapeDtypeStruct((gate.shape[0], rows.shape[1]), BF16),
        in_specs=[pl.BlockSpec(memory_space=pltpu.VMEM) for _ in range(4)],
        out_specs=pl.BlockSpec(memory_space=pltpu.VMEM),
        compiler_params=pltpu.CompilerParams(vmem_limit_bytes=60 * 1024 * 1024),
        name="shared_feed",
    )(rows, gain, gate, upward)


def copies_kernel(key_t, value_t, out):
    both = jnp.concatenate([key_t[...], value_t[...]], axis=0)
    for n in range(out.shape[0]):
        out[n] = both


def key_value_copies(key_t, value_t, count):
    head, width = key_t.shape
    return pl.pallas_call(
        copies_kernel,
        out_shape=jax.ShapeDtypeStruct((count, 2 * head, width), BF16),
        in_specs=[pl.BlockSpec(memory_space=pltpu.VMEM) for _ in range(2)],
        out_specs=pl.BlockSpec(memory_space=pltpu.VMEM),
        name="key_value_copies",
    )(key_t, value_t)


def final_kernel(share_hidden, sh_down, weight_high, weight_low, answers, updated, out):
    shared = lax.dot_general(
        share_hidden[...], sh_down[...], (((0,), (0,)), ((), ())), preferred_element_type=F32
    )
    rows = answers[...]
    routed = jnp.dot(weight_high[...], rows, preferred_element_type=F32) + jnp.dot(
        weight_low[...], rows, preferred_element_type=F32
    )
    out[...] = (updated[...].astype(F32) + shared + routed).astype(BF16)


def final_sum(*operands):
    return pl.pallas_call(
        final_kernel,
        out_shape=jax.ShapeDtypeStruct(operands[-1].shape, BF16),
        in_specs=[pl.BlockSpec(memory_space=pltpu.VMEM) for _ in operands],
        out_specs=pl.BlockSpec(memory_space=pltpu.VMEM),
        compiler_params=pltpu.CompilerParams(vmem_limit_bytes=24 * 1024 * 1024),
        name="final_sum",
    )(*operands)


def per_device(
    queries,
    keys,
    values,
    log_cum,
    residual,
    out_gain,
    w_out,
    ffn_gain,
    routes,
    route_weight,
    sh_gate,
    sh_up,
    sh_down,
    exp_gate,
    exp_up,
    exp_down,
):
    width, head = queries.shape
    near = ("zl", "x")
    whole = ("zh", "zl", "x")
    group = lax.axis_size(near)
    shards = lax.axis_size("tp")
    blocks = lax.axis_size(whole)
    team, own, shard = lax.axis_index("zh"), lax.axis_index(near), lax.axis_index("tp")
    hidden = sh_gate.shape[1]
    local_experts = exp_gate.shape[0]
    owners = shards // local_experts

    scale = head ** (-0.5)
    key_value = exchange(key_value_copies(keys.T, values.T, group), near)
    query = (queries.T.astype(F32) * scale).astype(BF16)
    teams = lax.axis_size("zh")
    moved = [
        lax.ppermute(query, "zh", [(i, (i + n) % teams) for i in range(teams)])
        for n in range(1, teams)
    ]
    query = jnp.stack([query, *moved])
    cum = lax.dynamic_slice_in_dim(log_cum, team * group * width, group * width, 1)
    expert_weights = packed_shards(
        jnp.swapaxes(exp_gate, 1, 2), jnp.swapaxes(exp_up, 1, 2), exp_down.reshape(-1, LANES)
    )
    expert_weights = lax.all_gather(expert_weights, "tp", axis=0, tiled=False)

    place = jnp.stack([team, own]).astype(jnp.int32)
    partial = partial_attention(place, key_value, query, cum)
    partial = exchange(partial, "zh")
    partial = partial.astype(F32)
    level = partial[:, head] + partial[:, head + 1] + partial[:, head + 2]
    share = jnp.exp(level - jnp.max(level, axis=0, keepdims=True))
    share = share / jnp.sum(share, axis=0, keepdims=True)
    head_out = jnp.sum(partial[:, :head] * share[:, None], axis=0).astype(BF16)

    all_heads = lax.all_gather(head_out[None], "tp", axis=0, tiled=True).astype(F32)
    channels = shards * head
    mean = jnp.sum(all_heads * all_heads, axis=(0, 1), keepdims=True) / channels
    inverse = lax.rsqrt(mean + EPS)
    mixed = (all_heads * inverse * out_gain.reshape(shards, head, 1)).astype(BF16).reshape(channels, width)
    attended = lax.dot_general(mixed, w_out, (((0,), (0,)), ((), ())), preferred_element_type=F32)
    updated = (residual.astype(F32) + attended).astype(BF16)
    all_rows = lax.all_gather(updated[None], "tp", axis=0, tiled=True)

    top = routes.shape[1]
    experts = local_experts * blocks
    capacity = 2 * width * top // experts
    slots = experts * capacity
    chosen = [routes[:, k, None] == lax.iota(jnp.int32, experts)[None, :] for k in range(top)]
    named = sum(c.astype(BF16) for c in chosen)
    earlier = (lax.iota(jnp.int32, width)[:, None] > lax.iota(jnp.int32, width)[None, :]).astype(BF16)
    rank = jnp.dot(earlier, named, preferred_element_type=F32)
    picks, turned = [], []
    for k in range(top):
        own = jnp.sum(jnp.where(chosen[k], rank, 0.0), axis=1).astype(jnp.int32)
        slot = routes[:, k] * capacity + own
        picks.append(slot[:, None] == lax.iota(jnp.int32, slots)[None, :])
        turned.append(lax.iota(jnp.int32, slots)[:, None] == slot[None, :])
    select = lax.optimization_barrier(sum(t.astype(BF16) for t in turned))
    weights = sum(jnp.where(p, route_weight[:, k, None], 0.0) for k, p in enumerate(picks))
    weight_high = lax.reduce_precision(weights, 8, 7)
    weight_low = (weights - weight_high).astype(BF16)
    weight_high = weight_high.astype(BF16)
    weight_high, weight_low = lax.optimization_barrier((weight_high, weight_low))

    outgoing = jnp.dot(select, updated, preferred_element_type=F32).astype(BF16)
    per_block = local_experts * capacity
    landed = exchange(outgoing.reshape(blocks, per_block, LANES), whole)
    rounds = blocks // owners
    landed = landed.reshape(rounds, owners, local_experts, capacity, LANES)
    landed = jnp.transpose(landed, (2, 1, 0, 3, 4)).reshape(shards, rounds * capacity, LANES)
    rows = exchange(landed, "tp")
    gain = ffn_gain.reshape(shards, 1, LANES)
    mine = (shard // owners).astype(jnp.int32)[None]
    routed_out = feed_forward(mine, rows, gain, expert_weights, hidden, local_experts)
    returned = exchange(routed_out, "tp")
    returned = returned.reshape(local_experts, owners, rounds, capacity, LANES)
    returned = jnp.transpose(returned, (2, 1, 0, 3, 4)).reshape(blocks, per_block, LANES)
    answers = exchange(returned, whole).reshape(slots, LANES)
    share_hidden = shared_feed(all_rows, gain, sh_gate.T, sh_up.T)
    share_hidden = lax.all_gather(share_hidden, "tp", axis=0, tiled=True)
    return final_sum(share_hidden, sh_down, weight_high, weight_low, answers, updated)


def solution(mesh):
    blocks, shards = mesh.devices.shape
    grid = Mesh(mesh.devices.reshape(*GRIDS[blocks], shards), ("zh", "zl", "x", "tp"))
    sp = ("zh", "zl", "x")
    in_specs = (
        P(sp, "tp"),
        P(sp, "tp"),
        P(sp, "tp"),
        P("tp", None),
        P(sp, "tp"),
        P(),
        P(None, "tp"),
        P(),
        P(sp, None),
        P(sp, None),
        P(None, "tp"),
        P(None, "tp"),
        P(None, "tp"),
        P(sp, None, "tp"),
        P(sp, None, "tp"),
        P(sp, None, "tp"),
    )
    return jax.shard_map(
        per_device, mesh=grid, in_specs=in_specs, out_specs=P(sp, "tp"), check_vma=False
    )
```
